32 devices in a mesh: sp: 8 (over z, x), tp: 4 (over y, core).
Axes of the slice: x: 2, y: 2, z: 4, core: 2. Of those that a mesh axis runs over, the one named last changes fastest.
Arguments:
- tokens: bfloat16 [6144, 2048], P(('sp', 'tp')), may hold values from -6 to 6
- norm_gain: bfloat16 [2048], replicated, may hold values from 0.099609375 to 1.8984375
- conv_value_w: bfloat16 [2048, 2048], P('sp', 'tp'), may hold values from -0.125 to 0.125
- conv_gate_w: bfloat16 [2048, 2048], P('sp', 'tp'), may hold values from -0.125 to 0.125
- rnn_input_w: bfloat16 [2048, 2560], P('sp', 'tp'), may hold values from -0.125 to 0.125
- rnn_gate_w: bfloat16 [2048, 2560], P('sp', 'tp'), may hold values from -0.125 to 0.125
- conv_kernel: bfloat16 [31, 2048], P(None, 'tp'), may hold values from -3 to 3
- conv_norm_gain: bfloat16 [2048], P('tp'), may hold values from 0.099609375 to 1.8984375
- conv_norm_shift: bfloat16 [2048], P('tp'), may hold values from -3 to 3
- short_kernel: bfloat16 [4, 2560], P(None, 'tp'), may hold values from -3 to 3
- recur_map: bfloat16 [16, 160, 160], P('tp'), may hold values from -0.5 to 0.5
- input_map: bfloat16 [16, 160, 160], P('tp'), may hold values from -0.5 to 0.5
- decay_param: float32 [2560], P('tp'), may hold values from 4.5 to 16
- decay_shift: float32 [6144, 16], P('sp', 'tp'), may hold values from -1.1 to 0
- initial_state: float32 [2560], P('tp'), may hold values from -5 to 5
- conv_out_w: bfloat16 [2048, 2048], P('tp', 'sp'), may hold values from -0.125 to 0.125
- rnn_out_w: bfloat16 [2560, 2048], P('tp', 'sp'), may hold values from -0.125 to 0.125
Outputs:
- mixed: bfloat16 [6144, 2048], P(('sp', 'tp'))
The draws below stay inside these ranges and needn't reach their ends.
All inputs are finite; a program needn't handle non-finite values.
Results may differ from the reference program's by a relative error of at most 0.015.
Values may be sent and summed in bfloat16 or wider, within the bound.
A program may use at most 128 MiB of HBM per device.

```python
import jax
import jax.numpy as jnp
from jax import lax

D = 2048
D_CONV = 2048
RNN_HEADS = 16
HEAD_DIM = 160
CONV_WIDTH = 31
SHORT_WIDTH = 4
TOK_DEV = 768
D_RNN = 2560
SEQUENCE_SPAN = 6144
N_TP = 4


def draw_conv_kernel(key, part):
    base = jnp.clip(jax.random.normal(jax.random.fold_in(key, 11), (CONV_WIDTH, D_CONV), jnp.float32), -4.0, 4.0)
    position = jnp.arange(D_CONV, dtype=jnp.float32) / D_CONV
    rough = jax.random.uniform(jax.random.fold_in(key, 12), (D_CONV,), jnp.float32, 0.5, 1.5)
    rising = jnp.exp(jnp.log(4.0) * position) / 2.0
    return (base * (rising * rough)[None, :] * CONV_WIDTH ** (-0.5)).astype(jnp.bfloat16)


def draw_decay_param(key, part):
    fast_heads = jax.random.randint(jax.random.fold_in(key, 21), (RNN_HEADS,), 0, 2) < 1
    fast_cols = jnp.repeat(fast_heads, HEAD_DIM)
    spread_draw = jax.random.uniform(jax.random.fold_in(key, 22), (D_RNN,), jnp.float32, 0.0, 1.0)
    slow_rate = jnp.exp(jnp.log(0.2) + spread_draw * jnp.log(4.0)) / SEQUENCE_SPAN
    fast_rate = jnp.exp(jnp.log(0.03) + spread_draw * jnp.log(0.08 / 0.03))
    rate = jnp.where(fast_cols, fast_rate, slow_rate)
    return -jnp.log(jnp.expm1(rate / 8.0))


def draw_decay_shift(key, part):
    sequence_indices = jnp.arange(SEQUENCE_SPAN, dtype=jnp.int32)
    span_len = max(TOK_DEV // 2, 1)
    span_count = (SEQUENCE_SPAN + span_len - 1) // span_len
    level_draw = jax.random.uniform(jax.random.fold_in(key, 31), (span_count,), jnp.float32, 0.0, 1.0)
    level = jnp.exp(jnp.log(0.1) + level_draw * jnp.log(10.0)) / SEQUENCE_SPAN
    baseline_amplitude = level[sequence_indices // span_len]
    spike_index = jax.random.randint(jax.random.fold_in(key, 32), (2,), 0, SEQUENCE_SPAN)
    objective_scalar = jax.random.uniform(jax.random.fold_in(key, 33), (2, RNN_HEADS), jnp.float32, 0.2, 0.4)
    match_tally = (sequence_indices[:, None] == spike_index[None, :]).astype(jnp.float32)
    spike_pattern = jnp.dot(match_tally, jnp.log1p(-objective_scalar))
    return spike_pattern - baseline_amplitude[:, None]


def steps_of(own_key, dims, pieces, low, top_value):
    gain = 1.0
    for dim, blocks in pieces:
        heights = jax.random.uniform(jax.random.fold_in(jax.random.fold_in(own_key, 6), dim), (blocks,), jnp.float32, low / len(pieces), top_value / len(pieces))
        gain = gain * jnp.repeat(jnp.exp(heights), dims[dim] // blocks).reshape((-1,) + (1,) * (len(dims) - 1 - dim))
    return gain


def scatter_about(own_key, shape, width, reach, split=(), kind=jnp.bfloat16):
    loudness = steps_of(own_key, shape, split, -0.22, 0.18) if split else 1.0
    drawn = jax.random.normal(own_key, shape, jnp.float32) * width * loudness
    return jnp.minimum(jnp.maximum(drawn, -reach), reach).astype(kind)


def setup_inputs(seed: int = 0) -> dict:
    key_list = jax.random.split(jax.random.key(seed), 18)
    tokens = scatter_about(key_list[0], (SEQUENCE_SPAN, D), 1.0, 6.0, ((0, 32),))
    norm_gain = jnp.clip(1.0 + 0.18 * jax.random.normal(key_list[1], (D,), jnp.float32), 0.099609375, 1.8984375).astype(jnp.bfloat16)
    conv_value_w = scatter_about(key_list[2], (D, D_CONV), D ** -0.5, 0.125, ((0, 8), (1, 4)))
    conv_gate_w = scatter_about(key_list[3], (D, D_CONV), D ** -0.5, 0.125, ((0, 8), (1, 4)))
    rnn_input_w = scatter_about(key_list[4], (D, D_RNN), D ** -0.5, 0.125, ((0, 8), (1, 4)))
    rnn_gate_w = scatter_about(key_list[5], (D, D_RNN), D ** -0.5, 0.125, ((0, 8), (1, 4)))
    conv_kernel = draw_conv_kernel(jax.random.fold_in(key_list[17], 71), 0)
    conv_norm_gain = jnp.clip(1.0 + 0.18 * jax.random.normal(key_list[7], (D_CONV,), jnp.float32), 0.099609375, 1.8984375).astype(jnp.bfloat16)
    conv_norm_shift = scatter_about(key_list[8], (D_CONV,), 0.5, 3.0, ((0, 4),))
    short_kernel = scatter_about(key_list[9], (SHORT_WIDTH, D_RNN), SHORT_WIDTH ** -0.5, 3.0, ((1, 4),))
    recur_map = scatter_about(key_list[10], (RNN_HEADS, HEAD_DIM, HEAD_DIM), HEAD_DIM ** -0.5, 0.5, ((0, 4),))
    input_map = scatter_about(key_list[11], (RNN_HEADS, HEAD_DIM, HEAD_DIM), HEAD_DIM ** -0.5, 0.5, ((0, 4),))
    decay_param = draw_decay_param(jax.random.fold_in(key_list[17], 71), 0)
    decay_shift = draw_decay_shift(jax.random.fold_in(key_list[17], 71), 0)
    initial_state = scatter_about(key_list[14], (D_RNN,), 1.0, 5.0, ((0, 4),), jnp.float32)
    conv_out_w = scatter_about(key_list[15], (D_CONV, D), D_CONV ** -0.5, 0.125, ((0, 4), (1, 8)))
    rnn_out_w = scatter_about(key_list[16], (D_RNN, D), D_RNN ** -0.5, 0.125, ((0, 4), (1, 8)))
    return dict(tokens=tokens, norm_gain=norm_gain, conv_value_w=conv_value_w, conv_gate_w=conv_gate_w, rnn_input_w=rnn_input_w, rnn_gate_w=rnn_gate_w, conv_kernel=conv_kernel, conv_norm_gain=conv_norm_gain, conv_norm_shift=conv_norm_shift, short_kernel=short_kernel, recur_map=recur_map, input_map=input_map, decay_param=decay_param, decay_shift=decay_shift, initial_state=initial_state, conv_out_w=conv_out_w, rnn_out_w=rnn_out_w)


EPS = 1e-06
EXPONENT = 8.0

def causal_taps(extended, kernel, length):
    result = jnp.zeros((length, extended.shape[1]), jnp.float32)
    for offset in range(kernel.shape[0]):
        result = result + kernel[offset].astype(jnp.float32) * extended[offset:offset + length]
    return result

def linear_pair(earlier, later):
    return (earlier[0] * later[0], later[0] * earlier[1] + later[1])

def block_diagonal(values, maps):
    row_count = values.shape[0]
    grouped = values.reshape(row_count, maps.shape[0], maps.shape[1]).astype(jnp.float32)
    mapped = jnp.einsum('rhi,hij->rhj', grouped, maps.astype(jnp.float32))
    return mapped.reshape(row_count, -1)

def reference(tokens, norm_gain, conv_value_w, conv_gate_w, rnn_input_w, rnn_gate_w, conv_kernel, conv_norm_gain, conv_norm_shift, short_kernel, recur_map, input_map, decay_param, decay_shift, initial_state, conv_out_w, rnn_out_w):
    length = TOK_DEV
    block_count = SEQUENCE_SPAN // length
    conv_reach = CONV_WIDTH - 1
    short_reach = SHORT_WIDTH - 1
    soft_rate = jax.nn.softplus(-decay_param)
    conv_group = D_CONV // N_TP
    rnn_group = D_RNN // N_TP

    def advance(carried, inputs):
        value_tail, gate_tail, input_tail, state = carried
        block_rows, block_shift = inputs
        as_float = block_rows.astype(jnp.float32)
        scale = lax.rsqrt(lax.optimization_barrier(jnp.mean(as_float * as_float, axis=1, keepdims=True)) + EPS)
        normed = (as_float * scale * norm_gain.astype(jnp.float32)).astype(jnp.bfloat16)
        conv_value = jnp.dot(normed, conv_value_w, preferred_element_type=jnp.float32).astype(jnp.bfloat16)
        conv_gate = jnp.dot(normed, conv_gate_w, preferred_element_type=jnp.float32).astype(jnp.bfloat16)
        rnn_input = jnp.dot(normed, rnn_input_w, preferred_element_type=jnp.float32).astype(jnp.bfloat16)
        rnn_gate = jnp.dot(normed, rnn_gate_w, preferred_element_type=jnp.float32).astype(jnp.bfloat16)
        value_ext = jnp.concatenate([value_tail, conv_value], axis=0)
        gate_ext = jnp.concatenate([gate_tail, conv_gate], axis=0)
        input_ext = jnp.concatenate([input_tail, rnn_input], axis=0)
        gated_values = value_ext.astype(jnp.float32) * jax.nn.sigmoid(gate_ext.astype(jnp.float32))
        conv_mixed = causal_taps(gated_values, conv_kernel, length)
        average = lax.optimization_barrier(jnp.mean(conv_mixed, axis=1, keepdims=True))
        spread = lax.optimization_barrier(jnp.mean(conv_mixed * conv_mixed, axis=1, keepdims=True)) - average * average
        scaled = (conv_mixed - average) * lax.rsqrt(spread + EPS)
        scaled = scaled * conv_norm_gain.astype(jnp.float32) + conv_norm_shift.astype(jnp.float32)
        conv_hidden = jax.nn.silu(scaled).astype(jnp.bfloat16)
        rnn_short = causal_taps(input_ext.astype(jnp.float32), short_kernel, length).astype(jnp.bfloat16)
        recur_gate = jax.nn.sigmoid(block_diagonal(rnn_short, recur_map))
        input_gate = jax.nn.sigmoid(block_diagonal(rnn_short, input_map))
        shift_cols = jnp.repeat(block_shift, HEAD_DIM, axis=1)
        log_decay = -EXPONENT * recur_gate * soft_rate[None, :] + shift_cols
        drive = jnp.sqrt(-jnp.expm1(2.0 * log_decay)) * input_gate * rnn_short.astype(jnp.float32)
        cum_decay, cum_drive = lax.associative_scan(linear_pair, (jnp.exp(log_decay), drive), axis=0)
        states = cum_drive + cum_decay * state[None, :]
        rnn_hidden = (states * jax.nn.gelu(rnn_gate.astype(jnp.float32), approximate=True)).astype(jnp.bfloat16)
        result = jnp.zeros((length, D), jnp.float32)
        for group in range(N_TP):
            conv_lo = group * conv_group
            rnn_lo = group * rnn_group
            partial_value = jnp.dot(conv_hidden[:, conv_lo:conv_lo + conv_group], conv_out_w[conv_lo:conv_lo + conv_group], preferred_element_type=jnp.float32)
            partial_value = partial_value + jnp.dot(rnn_hidden[:, rnn_lo:rnn_lo + rnn_group], rnn_out_w[rnn_lo:rnn_lo + rnn_group], preferred_element_type=jnp.float32)
            rounded = lax.optimization_barrier(partial_value.astype(jnp.bfloat16))
            result = result + rounded.astype(jnp.float32)
        carried_next = (value_ext[value_ext.shape[0] - conv_reach:], gate_ext[gate_ext.shape[0] - conv_reach:], input_ext[input_ext.shape[0] - short_reach:], states[length - 1])
        return (carried_next, result.astype(jnp.bfloat16))
    start_carry = (jnp.zeros((conv_reach, D_CONV), jnp.bfloat16), jnp.zeros((conv_reach, D_CONV), jnp.bfloat16), jnp.zeros((short_reach, D_RNN), jnp.bfloat16), initial_state.astype(jnp.float32))
    blocks_in = (tokens.reshape(block_count, length, D), decay_shift.reshape(block_count, length, RNN_HEADS))
    final_carry, outputs = lax.scan(advance, start_carry, blocks_in)
    return outputs.reshape(SEQUENCE_SPAN, D)
```

```python
import functools

import jax
import jax.numpy as jnp
from jax import lax
from jax.experimental import pallas as pl
from jax.experimental.pallas import tpu as pltpu
from jax.sharding import PartitionSpec as P

EPS = 1e-06
EXPONENT = 8.0


def shifted(x, axis, by):
    peers = lax.axis_size(axis)
    pairs = [(i, i + by) for i in range(peers) if 0 <= i + by < peers]
    return lax.ppermute(x, axis, pairs)


def send_to(src, dst, send, recv, axis, peer):
    return pltpu.make_async_remote_copy(
        src_ref=src,
        dst_ref=dst,
        send_sem=send,
        recv_sem=recv,
        device_id={axis: peer},
        device_id_type=pl.DeviceIdType.MESH,
    )


def project_kernel(n, m, x_ref, w_ref, o_ref, blocks, piece, acc, ring_send, ring_recv, tok_send, tok_recv, own_sem):
    half = n // 2
    me = lax.axis_index("sp")
    lane = lax.axis_index("tp")
    at = jnp.where(me % 2 == 0, me // 2, n - 1 - me // 2)

    def device_at(place):
        place = lax.rem(place + 2 * n, n)
        return jnp.where(place < half, 2 * place, 2 * (n - 1 - place) + 1)

    right = device_at(at + 1)
    left = device_at(at - 1)
    barrier = pltpu.get_barrier_semaphore()
    for peer in (left, right):
        pl.semaphore_signal(barrier, inc=1, device_id={"sp": peer}, device_id_type=pl.DeviceIdType.MESH)
    for i in range(1, m):
        pl.semaphore_signal(
            barrier, inc=1, device_id={"tp": lax.rem(lane + i, m)}, device_id_type=pl.DeviceIdType.MESH
        )
    own_w = pltpu.make_async_copy(w_ref, blocks.at[me], own_sem.at[0])
    own_x = pltpu.make_async_copy(x_ref, piece.at[lane], own_sem.at[1])
    own_w.start()
    own_x.start()
    own_w.wait()
    own_x.wait()
    pl.semaphore_wait(barrier, 2 + m - 1)
    rows = w_ref.shape[0] // 2

    def hop(way, k, part=None):
        slot = device_at(at - (k - 1)) if way == 0 else device_at(at + (k - 1))
        ref = blocks.at[slot] if part is None else blocks.at[slot, pl.ds(part * rows, rows)]
        return send_to(
            ref, ref, ring_send.at[way, k - 1], ring_recv.at[way, k - 1], "sp", right if way == 0 else left
        )

    tokens_out = [
        send_to(x_ref, piece.at[lane], tok_send.at[i - 1], tok_recv.at[i - 1], "tp", lax.rem(lane + i, m))
        for i in range(1, m)
    ]

    def add(slot, first=False):
        def one(j, _):
            here = pl.ds(pl.multiple_of(j * piece.shape[2], piece.shape[2]), piece.shape[2])
            term = jnp.dot(piece[j, slot], blocks[slot], preferred_element_type=jnp.float32)
            acc[here, :] = term if first else acc[here, :] + term
            return 0

        lax.fori_loop(0, m, one, 0)

    hop(0, 1).start()
    hop(1, 1).start()
    for copy in tokens_out:
        copy.start()
    hop(0, 1).wait_recv()
    hop(1, 1).wait_recv()
    hop(0, 2).start()
    hop(1, 2).start()
    for copy in tokens_out:
        copy.wait_recv()
    add(me, True)

    def step(k, _):
        add(device_at(at - (k - 1)))
        add(device_at(at + (k - 1)))
        hop(0, k).wait_recv()
        hop(1, k).wait_recv()

        @pl.when(k + 1 < half)
        def _():
            hop(0, k + 1).start()
            hop(1, k + 1).start()

        return 0

    lax.fori_loop(2, half, step, 0)
    hop(0, half, 0).start()
    hop(1, half, 1).start()
    add(device_at(at - (half - 1)))
    add(device_at(at + (half - 1)))
    hop(0, half, 0).wait_recv()
    hop(1, half, 1).wait_recv()
    add(device_at(at + half))

    def finish(j, _):
        here = pl.ds(pl.multiple_of(j * piece.shape[2], piece.shape[2]), piece.shape[2])
        o_ref[here, :] = acc[here, :].astype(o_ref.dtype)
        return 0

    lax.fori_loop(0, m, finish, 0)

    def sent(k, _):
        hop(0, k).wait_send()
        hop(1, k).wait_send()
        return 0

    lax.fori_loop(1, half, sent, 0)
    hop(0, half, 0).wait_send()
    hop(1, half, 1).wait_send()
    for copy in tokens_out:
        copy.wait_send()


def project(normed, weight):
    n = lax.axis_size("sp")
    m = lax.axis_size("tp")
    rows = normed.shape[0]
    depth, columns = weight.shape
    sliced = normed.reshape(rows, n, depth).transpose(1, 0, 2)
    vmem = pl.BlockSpec(memory_space=pltpu.VMEM)
    return pl.pallas_call(
        functools.partial(project_kernel, n, m),
        out_shape=jax.ShapeDtypeStruct((rows * m, columns), jnp.bfloat16),
        in_specs=[vmem, vmem],
        out_specs=vmem,
        scratch_shapes=[
            pltpu.VMEM((n, depth, columns), jnp.bfloat16),
            pltpu.VMEM((m, n, rows, depth), jnp.bfloat16),
            pltpu.VMEM((rows * m, columns), jnp.float32),
            pltpu.SemaphoreType.DMA((2, n // 2)),
            pltpu.SemaphoreType.DMA((2, n // 2)),
            pltpu.SemaphoreType.DMA((m - 1,)),
            pltpu.SemaphoreType.DMA((m - 1,)),
            pltpu.SemaphoreType.DMA((2,)),
        ],
        cost_estimate=pl.CostEstimate(
            flops=2 * rows * m * depth * n * columns, bytes_accessed=90_000_000, transcendentals=0
        ),
        compiler_params=pltpu.CompilerParams(
            collective_id=0, has_side_effects=True, vmem_limit_bytes=50 * 1024 * 1024
        ),
    )(sliced, weight)


def spread_kernel(n, axis, x_ref, o_ref, send, recv):
    me = lax.axis_index(axis)
    barrier = pltpu.get_barrier_semaphore()

    def greet(i, _):
        pl.semaphore_signal(
            barrier, inc=1, device_id={axis: lax.rem(me + i, n)}, device_id_type=pl.DeviceIdType.MESH
        )
        return 0

    lax.fori_loop(1, n, greet, 0)
    pl.semaphore_wait(barrier, n - 1)

    def copy(i):
        return send_to(x_ref, o_ref.at[me], send.at[i - 1], recv.at[i - 1], axis, lax.rem(me + i, n))

    def start(i, _):
        copy(i).start()
        return 0

    def wait(i, _):
        copy(i).wait()
        return 0

    lax.fori_loop(1, n, start, 0)
    o_ref[pl.ds(me, 1)] = x_ref[...][None]
    lax.fori_loop(1, n, wait, 0)


def spread_over(x, axis, collective_id):
    n = lax.axis_size(axis)
    vmem = pl.BlockSpec(memory_space=pltpu.VMEM)
    return pl.pallas_call(
        functools.partial(spread_kernel, n, axis),
        out_shape=jax.ShapeDtypeStruct((n,) + x.shape, x.dtype),
        in_specs=[vmem],
        out_specs=vmem,
        scratch_shapes=[pltpu.SemaphoreType.DMA((n - 1,)), pltpu.SemaphoreType.DMA((n - 1,))],
        cost_estimate=pl.CostEstimate(flops=0, bytes_accessed=10_000_000, transcendentals=0),
        compiler_params=pltpu.CompilerParams(
            collective_id=collective_id, has_side_effects=True, vmem_limit_bytes=4 * 1024 * 1024
        ),
    )(x)


def scan_kernel(parts, a_ref, b_ref, p_ref, h_ref):
    length, width = a_ref.shape
    run = length // parts
    cols = [slice(None)]

    def one(i, state):
        place = pl.ds(i, parts, stride=run)
        new = []
        for c, (p, h) in zip(cols, state):
            a = a_ref[place, c]
            h = a * h + b_ref[place, c]
            p = a * p
            p_ref[place, c] = p
            h_ref[place, c] = h
            new.append((p, h))
        return new

    first = [(jnp.ones((parts, width), jnp.float32), jnp.zeros((parts, width), jnp.float32)) for _ in cols]
    ends = lax.fori_loop(0, run, one, first)
    for c, (p, h) in zip(cols, ends):
        carry_p = p[0:1]
        carry_h = h[0:1]
        for s in range(1, parts):
            here = pl.ds(s * run, run)
            local_p = p_ref[here, c]
            h_ref[here, c] = h_ref[here, c] + local_p * carry_h
            p_ref[here, c] = local_p * carry_p
            carry_h = p[s : s + 1] * carry_h + h[s : s + 1]
            carry_p = p[s : s + 1] * carry_p


def scan(a, b):
    block = pl.BlockSpec((a.shape[0], 128), lambda c: (0, c))
    return pl.pallas_call(
        functools.partial(scan_kernel, 8),
        grid=(a.shape[1] // 128,),
        out_shape=[jax.ShapeDtypeStruct(a.shape, jnp.float32)] * 2,
        in_specs=[block, block],
        out_specs=[block, block],
        cost_estimate=pl.CostEstimate(flops=4 * a.size, bytes_accessed=16 * a.size, transcendentals=0),
        compiler_params=pltpu.CompilerParams(vmem_limit_bytes=20 * 1024 * 1024),
    )(a, b)


def entering(last_decay, last_drive, initial):
    n = lax.axis_size("sp")
    place = lax.axis_index("sp")
    pair = jnp.stack([last_decay, last_drive])
    gathered = spread_over(jnp.pad(pair, ((0, 6), (0, 0))), "sp", 1)
    state = initial
    for i in range(n):
        state = jnp.where(i < place, gathered[i, 0] * state + gathered[i, 1], state)
    return state


def causal_taps(extended, kernel, length):
    result = jnp.zeros((length, extended.shape[1]), jnp.float32)
    for offset in range(kernel.shape[0]):
        result = result + kernel[offset].astype(jnp.float32) * extended[offset : offset + length]
    return result


def block_diagonal(values, maps):
    heads, size, _ = maps.shape
    rows = [
        jnp.pad(maps[h], ((0, 0), (h * size, (heads - 1 - h) * size))) for h in range(heads)
    ]
    return jnp.dot(values, jnp.concatenate(rows, axis=0), preferred_element_type=jnp.float32)


def local(
    tokens,
    norm_gain,
    conv_value_w,
    conv_gate_w,
    rnn_input_w,
    rnn_gate_w,
    conv_kernel,
    conv_norm_gain,
    conv_norm_shift,
    short_kernel,
    recur_map,
    input_map,
    decay_param,
    decay_shift,
    initial_state,
    conv_out_w,
    rnn_out_w,
):
    as_float = tokens.astype(jnp.float32)
    scale = lax.rsqrt(jnp.mean(as_float * as_float, axis=1, keepdims=True) + EPS)
    normed = (as_float * scale * norm_gain.astype(jnp.float32)).astype(jnp.bfloat16)
    edges = [0]
    for weight in (conv_value_w, conv_gate_w, rnn_input_w, rnn_gate_w):
        edges.append(edges[-1] + weight.shape[1])
    joined = project(
        normed, jnp.concatenate([conv_value_w, conv_gate_w, rnn_input_w, rnn_gate_w], axis=1)
    )
    conv_value, conv_gate, rnn_input, rnn_gate = [
        joined[:, edges[index] : edges[index + 1]] for index in range(4)
    ]
    out_weights = (
        lax.all_gather(conv_out_w, "sp", axis=1, tiled=True),
        lax.all_gather(rnn_out_w, "sp", axis=1, tiled=True),
    )
    length = conv_value.shape[0]
    conv_reach = conv_kernel.shape[0] - 1
    short_reach = short_kernel.shape[0] - 1
    tail = shifted(joined[length - conv_reach :, : edges[3]], "sp", 1)
    value_tail = tail[:, : edges[1]]
    gate_tail = tail[:, edges[1] : edges[2]]
    input_tail = tail[conv_reach - short_reach :, edges[2] :]
    value_ext = jnp.concatenate([value_tail, conv_value], axis=0)
    gate_ext = jnp.concatenate([gate_tail, conv_gate], axis=0)
    input_ext = jnp.concatenate([input_tail, rnn_input], axis=0)
    gated_values = value_ext.astype(jnp.float32) * jax.nn.sigmoid(gate_ext.astype(jnp.float32))
    conv_mixed = causal_taps(gated_values, conv_kernel, length)
    moments = lax.psum(
        (jnp.sum(conv_mixed, axis=1), jnp.sum(conv_mixed * conv_mixed, axis=1)), "tp"
    )
    channels = conv_mixed.shape[1] * lax.axis_size("tp")
    average = moments[0][:, None] / channels
    spread = moments[1][:, None] / channels - average * average
    scaled = (conv_mixed - average) * lax.rsqrt(spread + EPS)
    scaled = scaled * conv_norm_gain.astype(jnp.float32) + conv_norm_shift.astype(jnp.float32)
    conv_hidden = jax.nn.silu(scaled).astype(jnp.bfloat16)
    rnn_short = causal_taps(input_ext.astype(jnp.float32), short_kernel, length).astype(
        jnp.bfloat16
    )
    recur_gate = jax.nn.sigmoid(block_diagonal(rnn_short, recur_map))
    input_gate = jax.nn.sigmoid(block_diagonal(rnn_short, input_map))
    shift_cols = jnp.repeat(decay_shift, recur_map.shape[1], axis=1)
    log_decay = -EXPONENT * recur_gate * jax.nn.softplus(-decay_param)[None, :] + shift_cols
    drive = jnp.sqrt(-jnp.expm1(2.0 * log_decay)) * input_gate * rnn_short.astype(jnp.float32)
    cum_decay, cum_drive = scan(jnp.exp(log_decay), drive)
    state_before = entering(cum_decay[length - 1], cum_drive[length - 1], initial_state)
    states = cum_drive + cum_decay * state_before[None, :]
    rnn_hidden = (states * jax.nn.gelu(rnn_gate.astype(jnp.float32), approximate=True)).astype(
        jnp.bfloat16
    )
    return lax.psum_scatter(
        (
            jnp.dot(conv_hidden, out_weights[0], preferred_element_type=jnp.float32)
            + jnp.dot(rnn_hidden, out_weights[1], preferred_element_type=jnp.float32)
        ).astype(jnp.bfloat16),
        "tp",
        scatter_dimension=0,
        tiled=True,
    )


def fused_kernel(n, m, dims, *refs):
    depth, quarter, ca, cr, wid, heads, taps, short = dims
    (
        tok_ref, ngain_ref, wv_ref, wg_ref, wri_ref, wrg_ref, wco_ref, wro_ref, pc_hbm, pr_hbm, bd_hbm, sh_hbm,
        o_ref,
        NB, X, BC, BI, BG, BO, PC, PR, BD, SH, G, MIX, MS, MR, E, S, Z0, Z1, SHC, RG, HC, HR, SM, SR, PB, R,
        swap_send, swap_recv, par_send, par_recv, line_send, line_recv, sib_send, sib_recv,
        tok_send, tok_recv, tokf_send, tokf_recv, halo_send, halo_recv, mom_send, mom_recv,
        state_send, state_recv, rs_send, rs_recv, tail_sem,
    ) = refs
    f32, bf16 = jnp.float32, jnp.bfloat16
    na, nu = n // 2, m // 2
    length = quarter * m
    model = depth * n
    half = length // 2
    reach = taps - 1
    pad = -(-reach // 8) * 8
    lanes = 128
    ga, gr = ca // lanes, cr // lanes
    tiles = length // lanes
    sp = lax.axis_index("sp")
    tp = lax.axis_index("tp")
    a, b = sp // 2, sp % 2
    u, v = tp // 2, tp % 2
    same = b == v
    other = b != v
    spc = 2 * a + v
    tpc = 2 * u + b

    def at(s, t):
        return {"sp": s, "tp": t}

    def where_is(s, t):
        return at(2 * (s // 2) + t % 2, 2 * (t // 2) + s % 2)

    partner = at(2 * a + v, 2 * u + b)
    sibling = at(sp, 2 * u + 1 - v)

    def remote(src, dst, send, recv, dev):
        return pltpu.make_async_remote_copy(
            src_ref=src, dst_ref=dst, send_sem=send, recv_sem=recv, device_id=dev,
            device_id_type=pl.DeviceIdType.MESH,
        )

    barrier = pltpu.get_barrier_semaphore()
    me = sp * m + tp

    def greet(i, _):
        to = (me + i) % (n * m)
        pl.semaphore_signal(barrier, inc=1, device_id=at(to // m, to % m), device_id_type=pl.DeviceIdType.MESH)
        return 0

    lax.fori_loop(1, n * m, greet, 0)

    bufs = [BC, BI, BG, BO]
    parts = [
        [(wv_ref, lambda j: BC.at[j, :, pl.ds(0, ca)]), (wg_ref, lambda j: BC.at[j, :, pl.ds(ca, ca)])],
        [(wri_ref, lambda j: BI.at[j])],
        [(wrg_ref, lambda j: BG.at[j])],
        [(wco_ref, lambda j: BO.at[j, pl.ds(0, ca)]), (wro_ref, lambda j: BO.at[j, pl.ds(ca, cr)])],
    ]
    first = [0, 2, 3, 4]

    def each_part(s, act):
        for p, (src, dst) in enumerate(parts[s]):
            act(src, dst, first[s] + p)

    def bring_local(s):
        each_part(s, lambda src, dst, k: pltpu.make_async_copy(src, dst(spc), swap_recv.at[k]).start())

    def swapped(src, dst, k):
        return remote(src, dst(sp), swap_send.at[k], swap_recv.at[k], partner)

    def bring_remote(s):
        each_part(s, lambda src, dst, k: swapped(src, dst, k).start())

    def brought(s):
        @pl.when(same)
        def _():
            each_part(s, lambda src, dst, k: pltpu.make_async_copy(src, dst(spc), swap_recv.at[k]).wait())

        @pl.when(other)
        def _():
            each_part(s, lambda src, dst, k: swapped(src, dst, k).wait_recv())

    params = [(pc_hbm, PC), (pr_hbm, PR), (bd_hbm, BD)]

    @pl.when(same)
    def _():
        for s in range(4):
            bring_local(s)
        for k, (src, dst) in enumerate(params):
            pltpu.make_async_copy(src, dst, par_recv.at[k]).start()
        pltpu.make_async_copy(sh_hbm, SH, par_recv.at[3]).start()

    gain = ngain_ref[...].astype(f32)

    def norm(i, _):
        rows = pl.ds(pl.multiple_of(i * 32, 32), 32)
        t = tok_ref[rows, :].astype(f32)
        scale = lax.rsqrt(jnp.sum(t * t, axis=1, keepdims=True) * (1.0 / model) + EPS)
        y = (t * scale * gain).astype(bf16)
        NB[rows, :] = y

        @pl.when(same)
        def _():
            X[tp, rows, :] = y

        return 0

    lax.fori_loop(0, quarter // 32, norm, 0)
    pl.semaphore_wait(barrier, n * m - 1)

    def param_send(k):
        return remote(params[k][0], params[k][1], par_send.at[k], par_recv.at[k], sibling)

    shift_send = remote(sh_hbm, SH, par_send.at[3], par_recv.at[3], partner)

    @pl.when(other)
    def _():
        bring_remote(0)
        bring_remote(1)

    tok_peer = remote(
        NB, X.at[tp], tok_send.at[0], tok_recv.at[v], at(2 * a + 1 - b, 2 * u + b)
    )
    tok_sib = remote(NB, X.at[tp], tok_send.at[1], tok_recv.at[v], sibling)

    @pl.when(other)
    def _():
        tok_sib.start()

    tok_peer.start()

    @pl.when(same)
    def _():
        for k in range(3):
            param_send(k).start()

    @pl.when(other)
    def _():
        bring_remote(2)
        bring_remote(3)
        shift_send.start()

    def block(s, j):
        return bufs[s].at[j]

    def up(s, o):
        ref = block(s, 2 * o + v)
        return remote(ref, ref, line_send.at[s, 0, o], line_recv.at[s, o], at(2 * a + 2 + b, tp))

    def down(s, o):
        ref = block(s, 2 * o + v)
        return remote(ref, ref, line_send.at[s, 1, o], line_recv.at[s, o], at(2 * a - 2 + b, tp))

    def across(s, o, core):
        ref = block(s, 2 * o + core)
        return remote(ref, ref, sib_send.at[s, o], sib_recv.at[s, o], sibling)

    def own(s):
        brought(s)

        @pl.when(a + 1 < na)
        def _():
            up(s, a).start()

        @pl.when(a > 0)
        def _():
            down(s, a).start()

        across(s, a, v).start()

    def step(s, k):
        @pl.when(a - k >= 0)
        def _():
            up(s, a - k).wait_recv()

            @pl.when(a + 1 < na)
            def _():
                up(s, a - k).start()

            across(s, a - k, v).start()

        @pl.when(a + k < na)
        def _():
            down(s, a + k).wait_recv()

            @pl.when(a > 0)
            def _():
                down(s, a + k).start()

            across(s, a + k, v).start()

    def crossed(s):
        def one(o, _):
            across(s, o, 1 - v).wait_recv()
            return 0

        lax.fori_loop(0, na, one, 0)

    def tok_from(c):
        q = 2 * u + c
        return remote(NB, X.at[q], tok_send.at[0], tok_recv.at[c], sibling)

    def tok_forward(i, uu):
        ref = X.at[pl.ds(2 * uu, 2)]
        return remote(ref, ref, tokf_send.at[i - 1], tokf_recv.at[i - 1], at(sp, 2 * ((u + i) % nu) + v))

    own(0)
    own(1)
    if na > 1:
        step(0, 1)
    for c in range(2):

        @pl.when(jnp.logical_or(other, v != c))
        def _():
            tok_from(c).wait_recv()

    for i in range(1, nu):
        tok_forward(i, u).start()
    for k in range(2, na):
        step(0, k)
    own(2)
    if na > 1:
        step(1, 1)

    @pl.when(same)
    def _():
        for k, (src, dst) in enumerate(params):
            pltpu.make_async_copy(src, dst, par_recv.at[k]).wait()
        pltpu.make_async_copy(sh_hbm, SH, par_recv.at[3]).wait()

    @pl.when(other)
    def _():
        for k in range(3):
            param_send(k).wait_recv()
        shift_send.wait_recv()

    for i in range(1, nu):
        tok_forward(i, (u - i + nu) % nu).wait_recv()
    crossed(0)

    chunk = 256
    cols_a = ca // chunk

    def tokens_half(r):
        return X[pl.ds(r * nu, nu)].reshape(half, model)

    def conv_project(i, _):
        r, j = i // cols_a, i % cols_a
        x = tokens_half(r)
        at_v = pl.ds(pl.multiple_of(j * chunk, chunk), chunk)
        at_g = pl.ds(pl.multiple_of(ca + j * chunk, chunk), chunk)
        val = jnp.dot(x, BC[:, :, at_v].reshape(model, chunk), preferred_element_type=f32).astype(bf16)
        gate = jnp.dot(x, BC[:, :, at_g].reshape(model, chunk), preferred_element_type=f32).astype(bf16)
        out = val.astype(f32) * jax.nn.sigmoid(gate.astype(f32))
        rows = pl.ds(pl.multiple_of(pad + r * half, 8), half)
        for g in range(chunk // lanes):
            G[j * (chunk // lanes) + g, rows, :] = out[:, g * lanes : (g + 1) * lanes]
        return 0

    total = 2 * cols_a
    lax.fori_loop(0, total // 2, conv_project, 0)
    if na > 2:
        step(1, 2)
    lax.fori_loop(total // 2, total, conv_project, 0)
    behind = where_is(spc + 1, tpc)
    conv_halo = remote(
        G.at[:, pl.ds(length, pad)], G.at[:, pl.ds(0, pad)], halo_send.at[0], halo_recv.at[0], behind
    )
    rnn_halo = remote(
        E.at[:, pl.ds(length, 8)], E.at[:, pl.ds(0, 8)], halo_send.at[1], halo_recv.at[1], behind
    )

    @pl.when(spc + 1 < n)
    def _():
        conv_halo.start()

    for k in range(3, na):
        step(1, k)
    own(3)

    @pl.when(spc == 0)
    def _():
        G[:, 0:pad, :] = jnp.zeros((ga, pad, lanes), f32)
        E[:, 0:8, :] = jnp.zeros((gr, 8, lanes), f32)

    @pl.when(spc > 0)
    def _():
        conv_halo.wait_recv()

    lane = lax.broadcasted_iota(jnp.int32, (lanes, lanes), 1)
    sub = lax.broadcasted_iota(jnp.int32, (lanes, lanes), 0)

    def convolve(i, _):
        t0 = pl.multiple_of(i * lanes, lanes)
        sums = jnp.zeros((lanes, lanes), f32)
        squares = jnp.zeros((lanes, lanes), f32)
        for g in range(ga):
            here = slice(g * lanes, (g + 1) * lanes)
            acc = jnp.zeros((lanes, lanes), f32)
            for k in range(taps):
                acc = acc + PC[k : k + 1, here] * G[g, pl.ds(t0 + (pad - reach + k), lanes), :]
            MIX[g, pl.ds(t0, lanes), :] = acc
            sums = sums + acc
            squares = squares + acc * acc
        s1 = jnp.sum(sums, axis=1, keepdims=True)
        s2 = jnp.sum(squares, axis=1, keepdims=True)
        both = jnp.where(lane == 0, s1, jnp.where(lane == 1, s2, 0.0))
        MS[i] = both.T[0:8, :]
        return 0

    lax.fori_loop(0, tiles // 2, convolve, 0)
    if na > 1:
        step(2, 1)
    lax.fori_loop(tiles // 2, tiles, convolve, 0)

    def moments(i):
        return remote(
            MS, MR.at[i - 1], mom_send.at[i - 1], mom_recv.at[i - 1], where_is(spc, (tpc + i) % m)
        )

    for k in range(2, min(3, na)):
        step(2, k)
    for i in range(1, m):
        moments(i).start()
    crossed(1)

    spans = []
    left = 0
    while left < cr:
        spans.append((left, min(chunk, cr - left)))
        left += chunk

    def input_project(r, _):
        x = tokens_half(r)
        rows = pl.ds(pl.multiple_of(8 + r * half, 8), half)
        for lo, size in spans:
            out = jnp.dot(x, BI[:, :, lo : lo + size].reshape(model, size), preferred_element_type=f32)
            out = out.astype(bf16).astype(f32)
            for g in range(size // lanes):
                E[lo // lanes + g, rows, :] = out[:, g * lanes : (g + 1) * lanes]
        return 0

    lax.fori_loop(0, 2, input_project, 0)

    @pl.when(spc + 1 < n)
    def _():
        rnn_halo.start()

    for k in range(3, na):
        step(2, k)

    def shift_columns(i, _):
        full = jnp.concatenate([SH[i], jnp.zeros((lanes - 8, lanes), f32)], axis=0)
        SHC[pl.ds(pl.multiple_of(i * lanes, lanes), lanes), :] = full.T
        return 0

    lax.fori_loop(0, tiles, shift_columns, 0)

    @pl.when(spc > 0)
    def _():
        rnn_halo.wait_recv()

    def short_conv(i, _):
        t0 = pl.multiple_of(i * lanes, lanes)
        for g in range(gr):
            here = slice(g * lanes, (g + 1) * lanes)
            acc = jnp.zeros((lanes, lanes), f32)
            for k in range(short):
                acc = acc + PR[k : k + 1, here] * E[g, pl.ds(t0 + (8 - short + 1 + k), lanes), :]
            S[pl.ds(t0, lanes), here] = acc.astype(bf16)
        return 0

    lax.fori_loop(0, tiles, short_conv, 0)

    def gate_maps(r, _):
        rows = pl.ds(pl.multiple_of(r * half, half), half)
        s = S[rows, :]
        Z0[rows, :] = jnp.dot(s, BD[0], preferred_element_type=f32)
        Z1[rows, :] = jnp.dot(s, BD[1], preferred_element_type=f32)
        return 0

    lax.fori_loop(0, 2, gate_maps, 0)
    if na > 1:
        step(3, 1)

    size = 32
    subs = size // 8
    head = cr // heads
    lane32 = lax.broadcasted_iota(jnp.int32, (size, lanes), 1)
    row8 = lax.broadcasted_iota(jnp.int32, (subs, 8, lanes), 1)

    def recur(i, carry):
        rows = pl.ds(pl.multiple_of(i * size, size), size)
        shc = SHC[rows, :]
        new = []
        for g in range(gr):
            here = slice(g * lanes, (g + 1) * lanes)
            shift = None
            for h in reversed(range((g * lanes) // head, (g * lanes + lanes - 1) // head + 1)):
                col = jnp.broadcast_to(shc[:, h : h + 1], (size, lanes))
                shift = col if shift is None else jnp.where(lane32 < (h + 1) * head - g * lanes, col, shift)
            log_decay = PR[short : short + 1, here] * jax.nn.sigmoid(Z0[rows, here]) + shift
            t = jnp.tanh(log_decay)
            drive = jnp.sqrt((-2.0 * t) / (1.0 - t)) * jax.nn.sigmoid(Z1[rows, here])
            drive = drive * S[rows, here].astype(f32)
            p = jnp.exp(log_decay).reshape(subs, 8, lanes)
            h_ = drive.reshape(subs, 8, lanes)
            for d in (1, 2, 4):
                keep = row8 >= d
                ps = jnp.where(keep, pltpu.roll(p, d, 1), 1.0)
                hs = jnp.where(keep, pltpu.roll(h_, d, 1), 0.0)
                h_ = p * hs + h_
                p = p * ps
            Z0[rows, here] = p.reshape(size, lanes)
            Z1[rows, here] = h_.reshape(size, lanes)
            pc, hc = carry[g]
            for q in range(subs):
                pe = p[q, 7:8, :]
                hc = pe * hc + h_[q, 7:8, :]
                pc = pe * pc
            new.append((pc, hc))
        return new

    start = [(jnp.ones((1, lanes), f32), jnp.zeros((1, lanes), f32)) for _ in range(gr)]
    ends = lax.fori_loop(0, length // size, recur, start)
    for g in range(gr):
        here = slice(g * lanes, (g + 1) * lanes)
        SM[0:1, here] = ends[g][0]
        SM[1:2, here] = ends[g][1]
    SM[2:8, :] = jnp.zeros((6, cr), f32)

    def state_to(i):
        return remote(SM, SR.at[spc], state_send.at[i - 1], state_recv.at[i - 1], where_is(spc + i, tpc))

    def state_from(i):
        return remote(SM, SR.at[spc - i], state_send.at[i - 1], state_recv.at[i - 1], where_is(spc, tpc))

    for i in range(1, n):

        @pl.when(spc + i < n)
        def _():
            state_to(i).start()

    crossed(2)

    def gate_project(r, _):
        x = tokens_half(r)
        rows = pl.ds(pl.multiple_of(r * half, half), half)
        for lo, size_ in spans:
            out = jnp.dot(x, BG[:, :, lo : lo + size_].reshape(model, size_), preferred_element_type=f32)
            RG[rows, lo : lo + size_] = out.astype(bf16)
        return 0

    lax.fori_loop(0, 2, gate_project, 0)
    for i in range(1, m):
        moments(i).wait_recv()

    def conv_finish(i, _):
        tot = MS[i]
        for p in range(m - 1):
            tot = tot + MR[p, i]
        average = tot[0:1, :] * (1.0 / (ca * m))
        spread = tot[1:2, :] * (1.0 / (ca * m)) - average * average
        inv = lax.rsqrt(spread + EPS)
        full = jnp.where(sub == 0, average, jnp.where(sub == 1, inv, 0.0)).T
        rows = pl.ds(pl.multiple_of(i * lanes, lanes), lanes)
        av, iv = full[:, 0:1], full[:, 1:2]
        for g in range(ga):
            here = slice(g * lanes, (g + 1) * lanes)
            y = (MIX[g, rows, :] - av) * iv * PC[taps : taps + 1, here] + PC[taps + 1 : taps + 2, here]
            HC[rows, here] = (y * jax.nn.sigmoid(y)).astype(bf16)
        return 0

    lax.fori_loop(0, tiles, conv_finish, 0)
    for i in range(1, n):

        @pl.when(spc - i >= 0)
        def _():
            state_from(i).wait_recv()

    def enter(i, state):
        return SR[i, 0:1, :] * state + SR[i, 1:2, :]

    before = lax.fori_loop(0, spc, enter, PR[short + 1 : short + 2, :])

    def rnn_finish(i, carry):
        rows = pl.ds(pl.multiple_of(i * size, size), size)
        new = []
        for g in range(gr):
            here = slice(g * lanes, (g + 1) * lanes)
            p = Z0[rows, here]
            h_ = Z1[rows, here]
            hc = carry[g]
            outs = []
            for q in range(subs):
                st = p[8 * q : 8 * q + 8] * hc + h_[8 * q : 8 * q + 8]
                outs.append(st)
                hc = st[7:8, :]
            new.append(hc)
            st = jnp.concatenate(outs, axis=0)
            gate = RG[rows, here].astype(f32)
            HR[rows, here] = (st * jax.nn.gelu(gate, approximate=True)).astype(bf16)
        return new

    lax.fori_loop(0, length // size, rnn_finish, [before[:, g * lanes : (g + 1) * lanes] for g in range(gr)])

    def out_copy(j, q):
        return remote(PB.at[j, q], R.at[tpc, j], rs_send.at[j, q], rs_recv.at[j, tpc], at(2 * a + v, q))

    def out_from(j, t):
        return remote(PB.at[j, 0], R.at[t, j], rs_send.at[j, 0], rs_recv.at[j, t], sibling)

    def out_block(j):
        y = jnp.dot(HC[...], BO[j, 0:ca], preferred_element_type=f32)
        y = (y + jnp.dot(HR[...], BO[j, ca : ca + cr], preferred_element_type=f32)).astype(bf16)
        PB[j] = y.reshape(m, quarter, wid)
        for q in range(m):
            mine = jnp.logical_and(same, tp == q)

            @pl.when(jnp.logical_not(mine))
            def _():
                out_copy(j, q).start()

            @pl.when(mine)
            def _():
                R[tpc, j] = y[q * quarter : (q + 1) * quarter]

    def settle(j):
        y = jnp.zeros((quarter, wid), f32)
        for t in range(m):

            @pl.when(jnp.logical_or(other, tpc != t))
            def _():
                out_from(j, t).wait_recv()

        for t in range(m):
            y = y + R[t, j].astype(f32)
        o_ref[:, pl.ds(pl.multiple_of(j * wid, wid), wid)] = y.astype(o_ref.dtype)

    def each_block(k, act):
        def one(i, _):
            o = jnp.where(i < 2, a - k, a + k)
            core = jnp.where(i % 2 == 0, v, 1 - v)
            ok = jnp.where(i < 2, a - k >= 0, jnp.logical_and(a + k < na, k > 0))

            @pl.when(ok)
            def _():
                act(o, 2 * o + core, i % 2)

            return 0

        lax.fori_loop(0, 4, one, 0)

    def produce(o, j, far):
        @pl.when(far == 1)
        def _():
            across(3, o, 1 - v).wait_recv()

        out_block(j)

    def outer(k, _):
        @pl.when(k >= 2)
        def _():
            step(3, k)

        each_block(k, produce)

        @pl.when(k >= 1)
        def _():
            each_block(k - 1, lambda o, j, far: settle(j))

        return 0

    lax.fori_loop(0, na, outer, 0)
    each_block(na - 1, lambda o, j, far: settle(j))

    def drain(o, _):
        for s in range(4):

            @pl.when(jnp.logical_and(o <= a, a + 1 < na))
            def _():
                up(s, o).wait_send()

            @pl.when(jnp.logical_and(o >= a, a > 0))
            def _():
                down(s, o).wait_send()

            across(s, o, v).wait_send()
        return 0

    lax.fori_loop(0, na, drain, 0)

    @pl.when(other)
    def _():
        for s in range(4):
            each_part(s, lambda src, dst, k: swapped(src, dst, k).wait_send())
        shift_send.wait_send()
        tok_sib.wait_send()

    @pl.when(same)
    def _():
        for k in range(3):
            param_send(k).wait_send()

    tok_peer.wait_send()
    for i in range(1, nu):
        tok_forward(i, u).wait_send()

    @pl.when(spc + 1 < n)
    def _():
        conv_halo.wait_send()
        rnn_halo.wait_send()

    for i in range(1, m):
        moments(i).wait_send()
    for i in range(1, n):

        @pl.when(spc + i < n)
        def _():
            state_to(i).wait_send()

    def drain_out(j, _):
        for q in range(m):

            @pl.when(jnp.logical_not(jnp.logical_and(same, tp == q)))
            def _():
                out_copy(j, q).wait_send()

        return 0

    lax.fori_loop(0, n, drain_out, 0)


def fused(
    tokens, norm_gain, conv_value_w, conv_gate_w, rnn_input_w, rnn_gate_w, conv_kernel, conv_norm_gain,
    conv_norm_shift, short_kernel, recur_map, input_map, decay_param, decay_shift, initial_state, conv_out_w,
    rnn_out_w,
):
    n = lax.axis_size("sp")
    m = lax.axis_size("tp")
    f32, bf16 = jnp.float32, jnp.bfloat16
    quarter, model = tokens.shape
    depth, ca = conv_value_w.shape
    cr = rnn_input_w.shape[1]
    wid = conv_out_w.shape[1]
    heads = recur_map.shape[0]
    taps, short = conv_kernel.shape[0], short_kernel.shape[0]
    length = quarter * m
    tiles = length // 128
    pad = -(-(taps - 1) // 8) * 8
    pc_rows = -(-(taps + 2) // 8) * 8
    pc = jnp.concatenate([conv_kernel, conv_norm_gain[None], conv_norm_shift[None]], axis=0).astype(f32)
    pc = jnp.pad(pc, ((0, pc_rows - taps - 2), (0, 0)))
    rate = -EXPONENT * jax.nn.softplus(-decay_param)
    pr = jnp.concatenate([short_kernel.astype(f32), rate[None], initial_state[None]], axis=0)
    pr_rows = -(-(short + 2) // 8) * 8
    pr = jnp.pad(pr, ((0, pr_rows - short - 2), (0, 0)))
    bd = jnp.stack([spread_heads(recur_map), spread_heads(input_map)])
    sh = decay_shift.T.reshape(heads, tiles, 128).transpose(1, 0, 2)
    sh = jnp.pad(sh, ((0, 0), (0, 8 - heads), (0, 0)))
    vmem = pl.BlockSpec(memory_space=pltpu.VMEM)
    anyw = pl.BlockSpec(memory_space=pl.ANY)
    na, nu = n // 2, m // 2
    dma = pltpu.SemaphoreType.DMA
    dims = (depth, quarter, ca, cr, wid, heads, taps, short)
    return pl.pallas_call(
        functools.partial(fused_kernel, n, m, dims),
        out_shape=jax.ShapeDtypeStruct((quarter, model), bf16),
        in_specs=[vmem, vmem] + [anyw] * 10,
        out_specs=vmem,
        scratch_shapes=[
            pltpu.VMEM((quarter, model), bf16),
            pltpu.VMEM((m, quarter, model), bf16),
            pltpu.VMEM((n, depth, 2 * ca), bf16),
            pltpu.VMEM((n, depth, cr), bf16),
            pltpu.VMEM((n, depth, cr), bf16),
            pltpu.VMEM((n, ca + cr, wid), bf16),
            pltpu.VMEM((pc_rows, ca), f32),
            pltpu.VMEM((pr_rows, cr), f32),
            pltpu.VMEM((2, cr, cr), bf16),
            pltpu.VMEM((tiles, 8, 128), f32),
            pltpu.VMEM((ca // 128, pad + length, 128), f32),
            pltpu.VMEM((ca // 128, length, 128), f32),
            pltpu.VMEM((tiles, 8, 128), f32),
            pltpu.VMEM((m - 1, tiles, 8, 128), f32),
            pltpu.VMEM((cr // 128, 8 + length, 128), f32),
            pltpu.VMEM((length, cr), bf16),
            pltpu.VMEM((length, cr), f32),
            pltpu.VMEM((length, cr), f32),
            pltpu.VMEM((length, 128), f32),
            pltpu.VMEM((length, cr), bf16),
            pltpu.VMEM((length, ca), bf16),
            pltpu.VMEM((length, cr), bf16),
            pltpu.VMEM((8, cr), f32),
            pltpu.VMEM((n, 8, cr), f32),
            pltpu.VMEM((n, m, quarter, wid), bf16),
            pltpu.VMEM((m, n, quarter, wid), bf16),
            dma((6,)), dma((6,)), dma((4,)), dma((4,)),
            dma((4, 2, na)), dma((4, na)), dma((4, na)), dma((4, na)),
            dma((2,)), dma((2,)), dma((max(nu - 1, 1),)), dma((max(nu - 1, 1),)),
            dma((2,)), dma((2,)), dma((m - 1,)), dma((m - 1,)),
            dma((n - 1,)), dma((n - 1,)), dma((n, m)), dma((n, m)), dma((1,)),
        ],
        cost_estimate=pl.CostEstimate(
            flops=2 * length * (model * 2 * (ca + cr) + (ca + cr) * model), bytes_accessed=10_000_000,
            transcendentals=0,
        ),
        compiler_params=pltpu.CompilerParams(
            collective_id=7, has_side_effects=True, vmem_limit_bytes=60 * 1024 * 1024
        ),
    )(
        tokens, norm_gain[None], conv_value_w, conv_gate_w, rnn_input_w, rnn_gate_w, conv_out_w, rnn_out_w,
        pc, pr, bd, sh,
    )


def spread_heads(maps):
    heads, size, _ = maps.shape
    rows = [jnp.pad(maps[h], ((0, 0), (h * size, (heads - 1 - h) * size))) for h in range(heads)]
    return jnp.concatenate(rows, axis=0)


def fits(n, m, args):
    quarter, model = args[0].shape
    depth, ca = args[2].shape
    cr = args[4].shape[1]
    wid = args[15].shape[1]
    heads = args[10].shape[0]
    return (
        n % 2 == 0 and m % 2 == 0 and wid % 128 == 0 and ca % 256 == 0 and cr % 128 == 0 and depth % 16 == 0
        and quarter % 32 == 0 and (quarter * m) % 256 == 0 and heads <= 8
    )


def whole_program(*args):
    n = lax.axis_size("sp")
    m = lax.axis_size("tp")
    return fused(*args) if fits(n, m, args) else local(*args)


def solution(mesh):
    return jax.shard_map(
        whole_program,
        mesh=mesh,
        in_specs=(
            P(("sp", "tp"), None),
            P(),
            P("sp", "tp"),
            P("sp", "tp"),
            P("sp", "tp"),
            P("sp", "tp"),
            P(None, "tp"),
            P("tp"),
            P("tp"),
            P(None, "tp"),
            P("tp", None, None),
            P("tp", None, None),
            P("tp"),
            P("sp", "tp"),
            P("tp"),
            P("tp", "sp"),
            P("tp", "sp"),
        ),
        out_specs=P(("sp", "tp"), None),
        check_vma=False,
    )
```

```python
import functools

import jax
import jax.numpy as jnp
from jax import lax
from jax.experimental import pallas as pl
from jax.experimental.pallas import tpu as pltpu
from jax.sharding import PartitionSpec as P

EPS = 1e-06
EXPONENT = 8.0


def shifted(x, axis, by):
    peers = lax.axis_size(axis)
    pairs = [(i, i + by) for i in range(peers) if 0 <= i + by < peers]
    return lax.ppermute(x, axis, pairs)


def send_to(src, dst, send, recv, axis, peer):
    return pltpu.make_async_remote_copy(
        src_ref=src,
        dst_ref=dst,
        send_sem=send,
        recv_sem=recv,
        device_id={axis: peer},
        device_id_type=pl.DeviceIdType.MESH,
    )


def project_kernel(n, m, x_ref, w_ref, o_ref, blocks, piece, acc, ring_send, ring_recv, tok_send, tok_recv, own_sem):
    half = n // 2
    me = lax.axis_index("sp")
    lane = lax.axis_index("tp")
    at = jnp.where(me % 2 == 0, me // 2, n - 1 - me // 2)

    def device_at(place):
        place = lax.rem(place + 2 * n, n)
        return jnp.where(place < half, 2 * place, 2 * (n - 1 - place) + 1)

    right = device_at(at + 1)
    left = device_at(at - 1)
    barrier = pltpu.get_barrier_semaphore()
    for peer in (left, right):
        pl.semaphore_signal(barrier, inc=1, device_id={"sp": peer}, device_id_type=pl.DeviceIdType.MESH)
    for i in range(1, m):
        pl.semaphore_signal(
            barrier, inc=1, device_id={"tp": lax.rem(lane + i, m)}, device_id_type=pl.DeviceIdType.MESH
        )
    own_w = pltpu.make_async_copy(w_ref, blocks.at[me], own_sem.at[0])
    own_x = pltpu.make_async_copy(x_ref, piece.at[lane], own_sem.at[1])
    own_w.start()
    own_x.start()
    own_w.wait()
    own_x.wait()
    pl.semaphore_wait(barrier, 2 + m - 1)
    rows = w_ref.shape[0] // 2

    def hop(way, k, part=None):
        slot = device_at(at - (k - 1)) if way == 0 else device_at(at + (k - 1))
        ref = blocks.at[slot] if part is None else blocks.at[slot, pl.ds(part * rows, rows)]
        return send_to(
            ref, ref, ring_send.at[way, k - 1], ring_recv.at[way, k - 1], "sp", right if way == 0 else left
        )

    tokens_out = [
        send_to(x_ref, piece.at[lane], tok_send.at[i - 1], tok_recv.at[i - 1], "tp", lax.rem(lane + i, m))
        for i in range(1, m)
    ]

    def add(slot, first=False):
        def one(j, _):
            here = pl.ds(pl.multiple_of(j * piece.shape[2], piece.shape[2]), piece.shape[2])
            term = jnp.dot(piece[j, slot], blocks[slot], preferred_element_type=jnp.float32)
            acc[here, :] = term if first else acc[here, :] + term
            return 0

        lax.fori_loop(0, m, one, 0)

    hop(0, 1).start()
    hop(1, 1).start()
    for copy in tokens_out:
        copy.start()
    hop(0, 1).wait_recv()
    hop(1, 1).wait_recv()
    hop(0, 2).start()
    hop(1, 2).start()
    for copy in tokens_out:
        copy.wait_recv()
    add(me, True)

    def step(k, _):
        add(device_at(at - (k - 1)))
        add(device_at(at + (k - 1)))
        hop(0, k).wait_recv()
        hop(1, k).wait_recv()

        @pl.when(k + 1 < half)
        def _():
            hop(0, k + 1).start()
            hop(1, k + 1).start()

        return 0

    lax.fori_loop(2, half, step, 0)
    hop(0, half, 0).start()
    hop(1, half, 1).start()
    add(device_at(at - (half - 1)))
    add(device_at(at + (half - 1)))
    hop(0, half, 0).wait_recv()
    hop(1, half, 1).wait_recv()
    add(device_at(at + half))

    def finish(j, _):
        here = pl.ds(pl.multiple_of(j * piece.shape[2], piece.shape[2]), piece.shape[2])
        o_ref[here, :] = acc[here, :].astype(o_ref.dtype)
        return 0

    lax.fori_loop(0, m, finish, 0)

    def sent(k, _):
        hop(0, k).wait_send()
        hop(1, k).wait_send()
        return 0

    lax.fori_loop(1, half, sent, 0)
    hop(0, half, 0).wait_send()
    hop(1, half, 1).wait_send()
    for copy in tokens_out:
        copy.wait_send()


def project(normed, weight):
    n = lax.axis_size("sp")
    m = lax.axis_size("tp")
    rows = normed.shape[0]
    depth, columns = weight.shape
    sliced = normed.reshape(rows, n, depth).transpose(1, 0, 2)
    vmem = pl.BlockSpec(memory_space=pltpu.VMEM)
    return pl.pallas_call(
        functools.partial(project_kernel, n, m),
        out_shape=jax.ShapeDtypeStruct((rows * m, columns), jnp.bfloat16),
        in_specs=[vmem, vmem],
        out_specs=vmem,
        scratch_shapes=[
            pltpu.VMEM((n, depth, columns), jnp.bfloat16),
            pltpu.VMEM((m, n, rows, depth), jnp.bfloat16),
            pltpu.VMEM((rows * m, columns), jnp.float32),
            pltpu.SemaphoreType.DMA((2, n // 2)),
            pltpu.SemaphoreType.DMA((2, n // 2)),
            pltpu.SemaphoreType.DMA((m - 1,)),
            pltpu.SemaphoreType.DMA((m - 1,)),
            pltpu.SemaphoreType.DMA((2,)),
        ],
        cost_estimate=pl.CostEstimate(
            flops=2 * rows * m * depth * n * columns, bytes_accessed=90_000_000, transcendentals=0
        ),
        compiler_params=pltpu.CompilerParams(
            collective_id=0, has_side_effects=True, vmem_limit_bytes=50 * 1024 * 1024
        ),
    )(sliced, weight)


def spread_kernel(n, axis, x_ref, o_ref, send, recv):
    me = lax.axis_index(axis)
    barrier = pltpu.get_barrier_semaphore()

    def greet(i, _):
        pl.semaphore_signal(
            barrier, inc=1, device_id={axis: lax.rem(me + i, n)}, device_id_type=pl.DeviceIdType.MESH
        )
        return 0

    lax.fori_loop(1, n, greet, 0)
    pl.semaphore_wait(barrier, n - 1)

    def copy(i):
        return send_to(x_ref, o_ref.at[me], send.at[i - 1], recv.at[i - 1], axis, lax.rem(me + i, n))

    def start(i, _):
        copy(i).start()
        return 0

    def wait(i, _):
        copy(i).wait()
        return 0

    lax.fori_loop(1, n, start, 0)
    o_ref[pl.ds(me, 1)] = x_ref[...][None]
    lax.fori_loop(1, n, wait, 0)


def spread_over(x, axis, collective_id):
    n = lax.axis_size(axis)
    vmem = pl.BlockSpec(memory_space=pltpu.VMEM)
    return pl.pallas_call(
        functools.partial(spread_kernel, n, axis),
        out_shape=jax.ShapeDtypeStruct((n,) + x.shape, x.dtype),
        in_specs=[vmem],
        out_specs=vmem,
        scratch_shapes=[pltpu.SemaphoreType.DMA((n - 1,)), pltpu.SemaphoreType.DMA((n - 1,))],
        cost_estimate=pl.CostEstimate(flops=0, bytes_accessed=10_000_000, transcendentals=0),
        compiler_params=pltpu.CompilerParams(
            collective_id=collective_id, has_side_effects=True, vmem_limit_bytes=4 * 1024 * 1024
        ),
    )(x)


def scan_kernel(parts, a_ref, b_ref, p_ref, h_ref):
    length, width = a_ref.shape
    run = length // parts
    cols = [slice(None)]

    def one(i, state):
        place = pl.ds(i, parts, stride=run)
        new = []
        for c, (p, h) in zip(cols, state):
            a = a_ref[place, c]
            h = a * h + b_ref[place, c]
            p = a * p
            p_ref[place, c] = p
            h_ref[place, c] = h
            new.append((p, h))
        return new

    first = [(jnp.ones((parts, width), jnp.float32), jnp.zeros((parts, width), jnp.float32)) for _ in cols]
    ends = lax.fori_loop(0, run, one, first)
    for c, (p, h) in zip(cols, ends):
        carry_p = p[0:1]
        carry_h = h[0:1]
        for s in range(1, parts):
            here = pl.ds(s * run, run)
            local_p = p_ref[here, c]
            h_ref[here, c] = h_ref[here, c] + local_p * carry_h
            p_ref[here, c] = local_p * carry_p
            carry_h = p[s : s + 1] * carry_h + h[s : s + 1]
            carry_p = p[s : s + 1] * carry_p


def scan(a, b):
    block = pl.BlockSpec((a.shape[0], 128), lambda c: (0, c))
    return pl.pallas_call(
        functools.partial(scan_kernel, 8),
        grid=(a.shape[1] // 128,),
        out_shape=[jax.ShapeDtypeStruct(a.shape, jnp.float32)] * 2,
        in_specs=[block, block],
        out_specs=[block, block],
        cost_estimate=pl.CostEstimate(flops=4 * a.size, bytes_accessed=16 * a.size, transcendentals=0),
        compiler_params=pltpu.CompilerParams(vmem_limit_bytes=20 * 1024 * 1024),
    )(a, b)


def entering(last_decay, last_drive, initial):
    n = lax.axis_size("sp")
    place = lax.axis_index("sp")
    pair = jnp.stack([last_decay, last_drive])
    gathered = spread_over(jnp.pad(pair, ((0, 6), (0, 0))), "sp", 1)
    state = initial
    for i in range(n):
        state = jnp.where(i < place, gathered[i, 0] * state + gathered[i, 1], state)
    return state


def causal_taps(extended, kernel, length):
    result = jnp.zeros((length, extended.shape[1]), jnp.float32)
    for offset in range(kernel.shape[0]):
        result = result + kernel[offset].astype(jnp.float32) * extended[offset : offset + length]
    return result


def block_diagonal(values, maps):
    heads, size, _ = maps.shape
    rows = [
        jnp.pad(maps[h], ((0, 0), (h * size, (heads - 1 - h) * size))) for h in range(heads)
    ]
    return jnp.dot(values, jnp.concatenate(rows, axis=0), preferred_element_type=jnp.float32)


def local(
    tokens,
    norm_gain,
    conv_value_w,
    conv_gate_w,
    rnn_input_w,
    rnn_gate_w,
    conv_kernel,
    conv_norm_gain,
    conv_norm_shift,
    short_kernel,
    recur_map,
    input_map,
    decay_param,
    decay_shift,
    initial_state,
    conv_out_w,
    rnn_out_w,
):
    as_float = tokens.astype(jnp.float32)
    scale = lax.rsqrt(jnp.mean(as_float * as_float, axis=1, keepdims=True) + EPS)
    normed = (as_float * scale * norm_gain.astype(jnp.float32)).astype(jnp.bfloat16)
    edges = [0]
    for weight in (conv_value_w, conv_gate_w, rnn_input_w, rnn_gate_w):
        edges.append(edges[-1] + weight.shape[1])
    joined = project(
        normed, jnp.concatenate([conv_value_w, conv_gate_w, rnn_input_w, rnn_gate_w], axis=1)
    )
    conv_value, conv_gate, rnn_input, rnn_gate = [
        joined[:, edges[index] : edges[index + 1]] for index in range(4)
    ]
    out_weights = (
        lax.all_gather(conv_out_w, "sp", axis=1, tiled=True),
        lax.all_gather(rnn_out_w, "sp", axis=1, tiled=True),
    )
    length = conv_value.shape[0]
    conv_reach = conv_kernel.shape[0] - 1
    short_reach = short_kernel.shape[0] - 1
    tail = shifted(joined[length - conv_reach :, : edges[3]], "sp", 1)
    value_tail = tail[:, : edges[1]]
    gate_tail = tail[:, edges[1] : edges[2]]
    input_tail = tail[conv_reach - short_reach :, edges[2] :]
    value_ext = jnp.concatenate([value_tail, conv_value], axis=0)
    gate_ext = jnp.concatenate([gate_tail, conv_gate], axis=0)
    input_ext = jnp.concatenate([input_tail, rnn_input], axis=0)
    gated_values = value_ext.astype(jnp.float32) * jax.nn.sigmoid(gate_ext.astype(jnp.float32))
    conv_mixed = causal_taps(gated_values, conv_kernel, length)
    moments = lax.psum(
        (jnp.sum(conv_mixed, axis=1), jnp.sum(conv_mixed * conv_mixed, axis=1)), "tp"
    )
    channels = conv_mixed.shape[1] * lax.axis_size("tp")
    average = moments[0][:, None] / channels
    spread = moments[1][:, None] / channels - average * average
    scaled = (conv_mixed - average) * lax.rsqrt(spread + EPS)
    scaled = scaled * conv_norm_gain.astype(jnp.float32) + conv_norm_shift.astype(jnp.float32)
    conv_hidden = jax.nn.silu(scaled).astype(jnp.bfloat16)
    rnn_short = causal_taps(input_ext.astype(jnp.float32), short_kernel, length).astype(
        jnp.bfloat16
    )
    recur_gate = jax.nn.sigmoid(block_diagonal(rnn_short, recur_map))
    input_gate = jax.nn.sigmoid(block_diagonal(rnn_short, input_map))
    shift_cols = jnp.repeat(decay_shift, recur_map.shape[1], axis=1)
    log_decay = -EXPONENT * recur_gate * jax.nn.softplus(-decay_param)[None, :] + shift_cols
    drive = jnp.sqrt(-jnp.expm1(2.0 * log_decay)) * input_gate * rnn_short.astype(jnp.float32)
    cum_decay, cum_drive = scan(jnp.exp(log_decay), drive)
    state_before = entering(cum_decay[length - 1], cum_drive[length - 1], initial_state)
    states = cum_drive + cum_decay * state_before[None, :]
    rnn_hidden = (states * jax.nn.gelu(rnn_gate.astype(jnp.float32), approximate=True)).astype(
        jnp.bfloat16
    )
    return lax.psum_scatter(
        (
            jnp.dot(conv_hidden, out_weights[0], preferred_element_type=jnp.float32)
            + jnp.dot(rnn_hidden, out_weights[1], preferred_element_type=jnp.float32)
        ).astype(jnp.bfloat16),
        "tp",
        scatter_dimension=0,
        tiled=True,
    )


def fused_kernel(n, m, dims, *refs):
    depth, quarter, ca, cr, wid, heads, taps, short = dims
    (
        tok_ref, ngain_hbm, wv_ref, wg_ref, wri_ref, wrg_ref, wco_ref, wro_ref, taps_hbm, cgain_hbm, cshift_hbm,
        short_hbm, rmap_hbm, imap_hbm, decay_hbm, init_hbm, sh_hbm,
        o_ref,
        TB, NGB, NB, X, BC, BI, BG, BO, KB, CGB, CSB, SKB, RM, DPB, ISB, PK, PC, BD, SH, G, MIX, MS, MR, E, S, Z0, Z1, SHC, RG, HC, HR, SM, SR, PB, R,
        own_sem, swap_send, swap_recv, par_send, par_recv, line_send, line_recv, sib_send, sib_recv,
        tok_send, tok_recv, tokf_send, tokf_recv, halo_send, halo_recv, mom_send, mom_recv,
        state_send, state_recv, rs_send, rs_recv,
    ) = refs
    f32, bf16 = jnp.float32, jnp.bfloat16
    na, nu = n // 2, m // 2
    length = quarter * m
    model = depth * n
    half = length // 2
    reach = taps - 1
    pad = -(-reach // 8) * 8
    lanes = 128
    ga, gr = ca // lanes, cr // lanes
    tiles = length // lanes
    sp = lax.axis_index("sp")
    tp = lax.axis_index("tp")
    a, b = sp // 2, sp % 2
    u, v = tp // 2, tp % 2
    same = b == v
    other = b != v
    spc = 2 * a + v
    tpc = 2 * u + b

    def at(s, t):
        return {"sp": s, "tp": t}

    def where_is(s, t):
        return at(2 * (s // 2) + t % 2, 2 * (t // 2) + s % 2)

    partner = at(2 * a + v, 2 * u + b)
    sibling = at(sp, 2 * u + 1 - v)

    def remote(src, dst, send, recv, dev):
        return pltpu.make_async_remote_copy(
            src_ref=src, dst_ref=dst, send_sem=send, recv_sem=recv, device_id=dev,
            device_id_type=pl.DeviceIdType.MESH,
        )

    barrier = pltpu.get_barrier_semaphore()
    me = sp * m + tp

    def greet(i, _):
        to = (me + i) % (n * m)
        pl.semaphore_signal(barrier, inc=1, device_id=at(to // m, to % m), device_id_type=pl.DeviceIdType.MESH)
        return 0

    gets = [
        pltpu.make_async_copy(tok_ref, TB, own_sem.at[0]),
        pltpu.make_async_copy(ngain_hbm, NGB, own_sem.at[1]),
    ]
    for get in gets:
        get.start()
    lax.fori_loop(1, n * m, greet, 0)

    hw = wid // 2
    bufs = [
        lambda o, core: BC.at[2 * o + core],
        lambda o, core: BI.at[2 * o + core],
        lambda o, core: BG.at[2 * o + core],
        lambda o, core: BO.at[0, o, core],
        lambda o, core: BO.at[1, o, core],
    ]
    parts = [
        [(wv_ref, lambda j: BC.at[j, :, pl.ds(0, ca)]), (wg_ref, lambda j: BC.at[j, :, pl.ds(ca, ca)])],
        [(wri_ref, lambda j: BI.at[j])],
        [(wrg_ref, lambda j: BG.at[j])],
    ]
    for e in range(2):
        here = pl.ds(e * hw, hw)
        parts.append([
            (wco_ref.at[:, here], lambda j, e=e: BO.at[e, j // 2, j % 2, pl.ds(0, ca)]),
            (wro_ref.at[:, here], lambda j, e=e: BO.at[e, j // 2, j % 2, pl.ds(ca, cr)]),
        ])
    first = [0, 2, 3, 4, 6]

    def each_part(s, act):
        for p, (src, dst) in enumerate(parts[s]):
            act(src, dst, first[s] + p)

    def bring_local(s):
        each_part(s, lambda src, dst, k: pltpu.make_async_copy(src, dst(spc), swap_recv.at[k]).start())

    def swapped(src, dst, k):
        return remote(src, dst(sp), swap_send.at[k], swap_recv.at[k], partner)

    def bring_remote(s):
        each_part(s, lambda src, dst, k: swapped(src, dst, k).start())

    def brought(s):
        @pl.when(same)
        def _():
            each_part(s, lambda src, dst, k: pltpu.make_async_copy(src, dst(spc), swap_recv.at[k]).wait())

        @pl.when(other)
        def _():
            each_part(s, lambda src, dst, k: swapped(src, dst, k).wait_recv())

    params = [
        (taps_hbm, KB), (cgain_hbm, CGB), (cshift_hbm, CSB), (short_hbm, SKB), (decay_hbm, DPB), (init_hbm, ISB),
        (rmap_hbm, RM.at[0]), (imap_hbm, RM.at[1]),
    ]
    np_ = len(params)

    @pl.when(same)
    def _():
        for s in range(5):
            bring_local(s)
        for k, (src, dst) in enumerate(params):
            pltpu.make_async_copy(src, dst, par_recv.at[k]).start()
        pltpu.make_async_copy(sh_hbm, SH, par_recv.at[np_]).start()

    for get in gets:
        get.wait()
    gain = NGB[...].astype(f32).reshape(1, model)

    def norm(i, _):
        rows = pl.ds(pl.multiple_of(i * 32, 32), 32)
        t = TB[rows, :].astype(f32)
        scale = lax.rsqrt(jnp.sum(t * t, axis=1, keepdims=True) * (1.0 / model) + EPS)
        y = (t * scale * gain).astype(bf16)
        NB[rows, :] = y

        @pl.when(same)
        def _():
            X[tp, rows, :] = y

        return 0

    lax.fori_loop(0, quarter // 32, norm, 0)
    pl.semaphore_wait(barrier, n * m - 1)

    def param_send(k):
        return remote(params[k][0], params[k][1], par_send.at[k], par_recv.at[k], sibling)

    shift_send = remote(sh_hbm, SH, par_send.at[np_], par_recv.at[np_], partner)

    tok_peer = remote(NB, X.at[tp], tok_send.at[0], tok_recv.at[v], at(2 * a + 1 - b, 2 * u + b))
    tok_sib = remote(NB, X.at[tp], tok_send.at[1], tok_recv.at[v], sibling)

    @pl.when(other)
    def _():
        bring_remote(0)

    @pl.when(same)
    def _():
        tok_peer.start()
        for k in range(np_):
            param_send(k).start()

    def block(s, o, core):
        return bufs[s](o, core) if isinstance(s, int) else BO.at[s - 3, o, core]

    def up(s, o):
        ref = block(s, o, v)
        return remote(ref, ref, line_send.at[s, 0, o], line_recv.at[s, o], at(2 * a + 2 + b, tp))

    def down(s, o):
        ref = block(s, o, v)
        return remote(ref, ref, line_send.at[s, 1, o], line_recv.at[s, o], at(2 * a - 2 + b, tp))

    def across(s, o, core):
        ref = block(s, o, core)
        return remote(ref, ref, sib_send.at[s, o], sib_recv.at[s, o], sibling)

    low = a < na // 2

    def inward(s, k, act):
        @pl.when(jnp.logical_and(low, a - k >= 0))
        def _():
            act(up(s, a - k))

        @pl.when(jnp.logical_and(jnp.logical_not(low), a + k < na))
        def _():
            act(down(s, a + k))

    def outward(s, k, act):
        @pl.when(jnp.logical_and(jnp.logical_and(low, a > 0), a + k < na))
        def _():
            act(down(s, a + k))

        @pl.when(jnp.logical_and(jnp.logical_and(jnp.logical_not(low), a + 1 < na), a - k >= 0))
        def _():
            act(up(s, a - k))

    window = 2
    going_in, going_out = [], []

    def push(way, order, s, k):
        if len(order) >= window:
            way(*order[-window], lambda c: c.wait_send())
        way(s, k, lambda c: c.start())
        order.append((s, k))

    def push_in(s, k):
        push(inward, going_in, s, k)

    def push_out(s, k):
        push(outward, going_out, s, k)

    def hold(s):
        brought(s)
        across(s, a, v).start()

    def take(s, k):
        @pl.when(a - k >= 0)
        def _():
            up(s, a - k).wait_recv()
            across(s, a - k, v).start()

        @pl.when(a + k < na)
        def _():
            down(s, a + k).wait_recv()
            across(s, a + k, v).start()

    def crossed(s):
        def one(o, _):
            across(s, o, 1 - v).wait_recv()
            return 0

        lax.fori_loop(0, na, one, 0)

    def tok_from(c):
        q = 2 * u + c
        return remote(NB, X.at[q], tok_send.at[0], tok_recv.at[c], sibling)

    def tok_forward(i, uu, c):
        ref = X.at[2 * uu + c]
        return remote(ref, ref, tokf_send.at[i - 1, c], tokf_recv.at[i - 1, c], at(sp, 2 * ((u + i) % nu) + v))

    at_end = jnp.logical_or(a == 0, a == na - 1)

    def mids(f):
        return pl.when(jnp.logical_not(at_end))(f)

    def ends(f):
        return pl.when(at_end)(f)

    def token_relay(c):
        @pl.when(jnp.logical_or(other, v != c))
        def _():
            tok_from(c).wait_recv()

        for i in range(1, nu):
            tok_forward(i, u, c).start()

    hold(0)
    push_in(0, 0)
    push_out(0, 0)

    @pl.when(other)
    def _():
        bring_remote(1)
        tok_sib.start()
        tok_peer.start()

    hold(1)
    push_in(1, 0)
    push_out(1, 0)
    take(0, 1)
    push_in(0, 1)
    push_out(0, 1)
    token_relay(v)
    take(1, 1)
    push_in(1, 1)
    push_out(1, 1)
    token_relay(1 - v)

    @pl.when(other)
    def _():
        bring_remote(2)
        shift_send.start()
        bring_remote(3)
        bring_remote(4)

    take(0, 2)
    push_out(0, 2)

    @mids
    def _():
        take(1, 2)
        push_out(1, 2)

    hold(2)
    push_in(2, 0)

    @pl.when(same)
    def _():
        for k, (src, dst) in enumerate(params):
            pltpu.make_async_copy(src, dst, par_recv.at[k]).wait()
        pltpu.make_async_copy(sh_hbm, SH, par_recv.at[np_]).wait()

    @pl.when(other)
    def _():
        for k in range(np_):
            param_send(k).wait_recv()
        shift_send.wait_recv()

    head = cr // heads
    PC[0:taps, :] = KB[...].astype(f32)
    PK[0:1, 0:ca] = CGB[...].astype(f32).reshape(1, ca)
    PK[1:2, 0:ca] = CSB[...].astype(f32).reshape(1, ca)
    PK[2 : 2 + short, 0:cr] = SKB[...].astype(f32)
    x = -DPB[...].reshape(1, cr)
    z = jnp.exp(-jnp.abs(x))
    z = z / (2.0 + z)
    z2 = z * z
    series = jnp.full_like(z, 1.0 / 17.0)
    for k in range(15, 0, -2):
        series = series * z2 + 1.0 / k
    PK[2 + short : 3 + short, 0:cr] = -EXPONENT * (jnp.maximum(x, 0.0) + 2.0 * z * series)
    PK[3 + short : 4 + short, 0:cr] = ISB[...].reshape(1, cr)
    for g in range(2):
        BD[g] = jnp.zeros((cr, cr), bf16)
        for h in range(heads):
            BD[g, h * head : (h + 1) * head, h * head : (h + 1) * head] = RM[g, h]

    def shift_columns(i, _):
        cols = SH[:, pl.ds(pl.multiple_of(i * lanes, lanes), lanes)]
        full = jnp.concatenate([cols, jnp.zeros((lanes - heads, lanes), f32)], axis=0)
        SHC[pl.ds(pl.multiple_of(i * lanes, lanes), lanes), :] = full.T
        return 0

    lax.fori_loop(0, tiles, shift_columns, 0)

    @ends
    def _():
        take(0, 3)

    for i in range(1, nu):
        for c in range(2):
            tok_forward(i, (u - i + nu) % nu, c).wait_recv()
    crossed(0)

    chunk = 256
    cols_a = ca // chunk

    def tokens_half(r):
        return X[pl.ds(r * nu, nu)].reshape(half, model)

    def conv_project(i, _):
        r, j = i // cols_a, i % cols_a
        x = tokens_half(r)
        at_v = pl.ds(pl.multiple_of(j * chunk, chunk), chunk)
        at_g = pl.ds(pl.multiple_of(ca + j * chunk, chunk), chunk)
        val = jnp.dot(x, BC[:, :, at_v].reshape(model, chunk), preferred_element_type=f32).astype(bf16)
        gate = jnp.dot(x, BC[:, :, at_g].reshape(model, chunk), preferred_element_type=f32).astype(bf16)
        out = val.astype(f32) * jax.nn.sigmoid(gate.astype(f32))
        rows = pl.ds(pl.multiple_of(pad + r * half, 8), half)
        for g in range(chunk // lanes):
            G[j * (chunk // lanes) + g, rows, :] = out[:, g * lanes : (g + 1) * lanes]
        return 0

    lax.fori_loop(0, 2 * cols_a, conv_project, 0)
    behind = where_is(spc + 1, tpc)
    conv_halo = remote(
        G.at[:, pl.ds(length, pad)], G.at[:, pl.ds(0, pad)], halo_send.at[0], halo_recv.at[0], behind
    )
    rnn_halo = remote(
        E.at[:, pl.ds(length, 8)], E.at[:, pl.ds(0, 8)], halo_send.at[1], halo_recv.at[1], behind
    )

    @pl.when(spc + 1 < n)
    def _():
        conv_halo.start()

    @mids
    def _():
        push_out(2, 0)
        take(2, 1)

    push_in(2, 1)
    hold(3)
    push_in(3, 0)
    hold(4)
    push_in(4, 0)

    @pl.when(spc == 0)
    def _():
        G[:, 0:pad, :] = jnp.zeros((ga, pad, lanes), f32)
        E[:, 0:8, :] = jnp.zeros((gr, 8, lanes), f32)

    @pl.when(spc > 0)
    def _():
        conv_halo.wait_recv()

    @mids
    def _():
        push_out(2, 1)

    lane = lax.broadcasted_iota(jnp.int32, (lanes, lanes), 1)
    sub = lax.broadcasted_iota(jnp.int32, (lanes, lanes), 0)

    def convolve(i, _):
        t0 = pl.multiple_of(i * lanes, lanes)
        sums = jnp.zeros((lanes, lanes), f32)
        squares = jnp.zeros((lanes, lanes), f32)
        for g in range(ga):
            here = slice(g * lanes, (g + 1) * lanes)
            acc = jnp.zeros((lanes, lanes), f32)
            for k in range(taps):
                acc = acc + PC[k : k + 1, here] * G[g, pl.ds(t0 + (pad - reach + k), lanes), :]
            MIX[g, pl.ds(t0, lanes), :] = acc
            sums = sums + acc
            squares = squares + acc * acc
        s1 = jnp.sum(sums, axis=1, keepdims=True)
        s2 = jnp.sum(squares, axis=1, keepdims=True)
        both = jnp.where(lane == 0, s1, jnp.where(lane == 1, s2, 0.0))
        MS[i] = both.T[0:8, :]
        return 0

    lax.fori_loop(0, tiles, convolve, 0)

    def moments(i):
        return remote(
            MS, MR.at[i - 1], mom_send.at[i - 1], mom_recv.at[i - 1], where_is(spc, (tpc + i) % m)
        )

    for i in range(1, m):
        moments(i).start()

    @mids
    def _():
        take(2, 2)
        push_out(2, 2)

    @ends
    def _():
        take(1, 2)
        take(1, 3)

    crossed(1)

    spans = []
    left = 0
    while left < cr:
        spans.append((left, min(chunk, cr - left)))
        left += chunk

    def input_project(r, _):
        x = tokens_half(r)
        rows = pl.ds(pl.multiple_of(8 + r * half, 8), half)
        for lo, size in spans:
            out = jnp.dot(x, BI[:, :, lo : lo + size].reshape(model, size), preferred_element_type=f32)
            out = out.astype(bf16).astype(f32)
            for g in range(size // lanes):
                E[lo // lanes + g, rows, :] = out[:, g * lanes : (g + 1) * lanes]
        return 0

    lax.fori_loop(0, 2, input_project, 0)

    @pl.when(spc + 1 < n)
    def _():
        rnn_halo.start()

    @pl.when(spc > 0)
    def _():
        rnn_halo.wait_recv()

    def short_conv(i, _):
        t0 = pl.multiple_of(i * lanes, lanes)
        for g in range(gr):
            here = slice(g * lanes, (g + 1) * lanes)
            acc = jnp.zeros((lanes, lanes), f32)
            for k in range(short):
                acc = acc + PK[2 + k : 3 + k, here] * E[g, pl.ds(t0 + (8 - short + 1 + k), lanes), :]
            S[pl.ds(t0, lanes), here] = acc.astype(bf16)
        return 0

    lax.fori_loop(0, tiles, short_conv, 0)

    def gate_maps(r, _):
        rows = pl.ds(pl.multiple_of(r * half, half), half)
        s = S[rows, :]
        Z0[rows, :] = jnp.dot(s, BD[0], preferred_element_type=f32)
        Z1[rows, :] = jnp.dot(s, BD[1], preferred_element_type=f32)
        return 0

    lax.fori_loop(0, 2, gate_maps, 0)

    @mids
    def _():
        take(3, 1)
        push_out(3, 0)

    push_in(3, 1)

    size = 32
    subs = size // 8
    lane32 = lax.broadcasted_iota(jnp.int32, (size, lanes), 1)
    row8 = lax.broadcasted_iota(jnp.int32, (subs, 8, lanes), 1)

    def recur(i, carry):
        rows = pl.ds(pl.multiple_of(i * size, size), size)
        shc = SHC[rows, :]
        new = []
        for g in range(gr):
            here = slice(g * lanes, (g + 1) * lanes)
            shift = None
            for h in reversed(range((g * lanes) // head, (g * lanes + lanes - 1) // head + 1)):
                col = jnp.broadcast_to(shc[:, h : h + 1], (size, lanes))
                shift = col if shift is None else jnp.where(lane32 < (h + 1) * head - g * lanes, col, shift)
            log_decay = PK[2 + short : 3 + short, here] * jax.nn.sigmoid(Z0[rows, here]) + shift
            t = jnp.tanh(log_decay)
            drive = jnp.sqrt((-2.0 * t) / (1.0 - t)) * jax.nn.sigmoid(Z1[rows, here])
            drive = drive * S[rows, here].astype(f32)
            p = jnp.exp(log_decay).reshape(subs, 8, lanes)
            h_ = drive.reshape(subs, 8, lanes)
            for d in (1, 2, 4):
                keep = row8 >= d
                ps = jnp.where(keep, pltpu.roll(p, d, 1), 1.0)
                hs = jnp.where(keep, pltpu.roll(h_, d, 1), 0.0)
                h_ = p * hs + h_
                p = p * ps
            Z0[rows, here] = p.reshape(size, lanes)
            Z1[rows, here] = h_.reshape(size, lanes)
            pc, hc = carry[g]
            for q in range(subs):
                pe = p[q, 7:8, :]
                hc = pe * hc + h_[q, 7:8, :]
                pc = pe * pc
            new.append((pc, hc))
        return new

    start = [(jnp.ones((1, lanes), f32), jnp.zeros((1, lanes), f32)) for _ in range(gr)]
    last = lax.fori_loop(0, length // size, recur, start)
    for g in range(gr):
        here = slice(g * lanes, (g + 1) * lanes)
        SM[0:1, here] = last[g][0]
        SM[1:2, here] = last[g][1]
    SM[2:8, :] = jnp.zeros((6, cr), f32)

    def state_to(i):
        return remote(SM, SR.at[spc], state_send.at[i - 1], state_recv.at[i - 1], where_is(spc + i, tpc))

    def state_from(i):
        return remote(SM, SR.at[spc - i], state_send.at[i - 1], state_recv.at[i - 1], where_is(spc, tpc))

    for i in range(1, n):

        @pl.when(spc + i < n)
        def _():
            state_to(i).start()


    @mids
    def _():
        take(4, 1)
        push_out(3, 1)

    push_in(4, 1)
    for i in range(1, m):
        moments(i).wait_recv()

    def conv_finish(i, _):
        tot = MS[i]
        for p in range(m - 1):
            tot = tot + MR[p, i]
        average = tot[0:1, :] * (1.0 / (ca * m))
        spread = tot[1:2, :] * (1.0 / (ca * m)) - average * average
        inv = lax.rsqrt(spread + EPS)
        full = jnp.where(sub == 0, average, jnp.where(sub == 1, inv, 0.0)).T
        rows = pl.ds(pl.multiple_of(i * lanes, lanes), lanes)
        av, iv = full[:, 0:1], full[:, 1:2]
        for g in range(ga):
            here = slice(g * lanes, (g + 1) * lanes)
            y = (MIX[g, rows, :] - av) * iv * PK[0:1, here] + PK[1:2, here]
            HC[rows, here] = (y * jax.nn.sigmoid(y)).astype(bf16)
        return 0

    lax.fori_loop(0, tiles, conv_finish, 0)
    @ends
    def _():
        take(2, 1)
        take(2, 2)
        take(2, 3)

    crossed(2)

    def gate_project(r, _):
        x = tokens_half(r)
        rows = pl.ds(pl.multiple_of(r * half, half), half)
        for lo, size_ in spans:
            out = jnp.dot(x, BG[:, :, lo : lo + size_].reshape(model, size_), preferred_element_type=f32)
            RG[rows, lo : lo + size_] = out.astype(bf16)
        return 0

    lax.fori_loop(0, 2, gate_project, 0)
    for i in range(1, n):

        @pl.when(spc - i >= 0)
        def _():
            state_from(i).wait_recv()

    def enter(i, state):
        return SR[i, 0:1, :] * state + SR[i, 1:2, :]

    before = lax.fori_loop(0, spc, enter, PK[3 + short : 4 + short, 0:cr])

    def rnn_finish(i, carry):
        rows = pl.ds(pl.multiple_of(i * size, size), size)
        new = []
        for g in range(gr):
            here = slice(g * lanes, (g + 1) * lanes)
            p = Z0[rows, here]
            h_ = Z1[rows, here]
            hc = carry[g]
            outs = []
            for q in range(subs):
                st = p[8 * q : 8 * q + 8] * hc + h_[8 * q : 8 * q + 8]
                outs.append(st)
                hc = st[7:8, :]
            new.append(hc)
            st = jnp.concatenate(outs, axis=0)
            gate = RG[rows, here].astype(f32)
            HR[rows, here] = (st * jax.nn.gelu(gate, approximate=True)).astype(bf16)
        return new

    lax.fori_loop(0, length // size, rnn_finish, [before[:, g * lanes : (g + 1) * lanes] for g in range(gr)])

    @mids
    def _():
        take(3, 2)
        push_out(3, 2)

    def out_copy(e, o, q):
        return remote(
            PB.at[e, o, q], R.at[tpc, e, o], rs_send.at[e, o, q], rs_recv.at[e, o, tpc], at(2 * a + v, q)
        )

    def out_from(e, o, t):
        return remote(PB.at[e, o, 0], R.at[t, e, o], rs_send.at[e, o, 0], rs_recv.at[e, o, t], sibling)

    def produce(e, o):
        across(3 + e, o, 1 - v).wait_recv()
        w = jnp.concatenate([BO[e, o, 0], BO[e, o, 1]], axis=1)
        y = jnp.dot(HC[...], w[0:ca], preferred_element_type=f32)
        y = (y + jnp.dot(HR[...], w[ca : ca + cr], preferred_element_type=f32)).astype(bf16)
        PB[e, o] = y.reshape(m, quarter, wid)
        for q in range(m):
            mine = jnp.logical_and(same, tp == q)

            @pl.when(jnp.logical_not(mine))
            def _():
                out_copy(e, o, q).start()

            @pl.when(mine)
            def _():
                R[tpc, e, o] = y[q * quarter : (q + 1) * quarter]

    def settle(e, o):
        for t in range(m):

            @pl.when(jnp.logical_or(other, tpc != t))
            def _():
                out_from(e, o, t).wait_recv()

        y = R[0, e, o].astype(f32)
        for t in range(1, m):
            y = y + R[t, e, o].astype(f32)
        y = y.astype(o_ref.dtype)
        for c in range(2):
            lo = pl.multiple_of((2 * o + c) * wid + e * hw, hw)
            o_ref[:, pl.ds(lo, hw)] = y[:, c * hw : (c + 1) * hw]

    def each_origin(i, act):
        e = jnp.where(jnp.logical_or(i == 1, i > na), 1, 0)
        k = jnp.where(i < 2, 0, jnp.where(i <= na, i - 1, i - na))

        def one(t, _):
            o = jnp.where(t == 0, a - k, a + k)
            ok = jnp.where(t == 0, o >= 0, jnp.logical_and(o < na, k > 0))

            @pl.when(ok)
            def _():
                act(e, o)

            return 0

        def ready():
            @pl.when(jnp.logical_and(at_end, k > 0))
            def _():
                take(3 + e, k)

        return ready, lambda: lax.fori_loop(0, 2, one, 0)

    def outer(i, _):
        ready, run = each_origin(i, produce)
        ready()

        @pl.when(jnp.logical_and(jnp.logical_not(at_end), i == na + 2))
        def _():
            take(4, 2)

        run()

        @mids
        def _():
            for stage, k in ((na - 1, 0), (na + 1, 1), (na + 2, 2)):

                @pl.when(i == stage)
                def _():
                    push_out(4, k)

        @pl.when(jnp.logical_and(at_end, i >= 1))
        def _():
            each_origin(i - 1, settle)[1]()

        return 0

    lax.fori_loop(0, 2 * na, outer, 0)

    def conclude(i, _):
        each_origin(i, settle)[1]()
        return 0

    lax.fori_loop(jnp.where(at_end, 2 * na - 1, 0), 2 * na, conclude, 0)

    def drain(o, _):
        for s in range(5):
            across(s, o, v).wait_send()
        return 0

    assert len(going_in) == 10 and len(going_out) == 15
    lax.fori_loop(0, na, drain, 0)

    for way, order in ((inward, going_in), (outward, going_out)):
        for one in order[-window:]:
            way(*one, lambda c: c.wait_send())

    @pl.when(other)
    def _():
        for s in range(5):
            each_part(s, lambda src, dst, k: swapped(src, dst, k).wait_send())
        shift_send.wait_send()
        tok_sib.wait_send()

    @pl.when(same)
    def _():
        for k in range(np_):
            param_send(k).wait_send()

    tok_peer.wait_send()
    for i in range(1, nu):
        for c in range(2):
            tok_forward(i, u, c).wait_send()

    @pl.when(spc + 1 < n)
    def _():
        conv_halo.wait_send()
        rnn_halo.wait_send()

    for i in range(1, m):
        moments(i).wait_send()
    for i in range(1, n):

        @pl.when(spc + i < n)
        def _():
            state_to(i).wait_send()

    def drain_out(o, _):
        for e in range(2):
            for q in range(m):

                @pl.when(jnp.logical_not(jnp.logical_and(same, tp == q)))
                def _():
                    out_copy(e, o, q).wait_send()

        return 0

    lax.fori_loop(0, na, drain_out, 0)


def fused(
    tokens, norm_gain, conv_value_w, conv_gate_w, rnn_input_w, rnn_gate_w, conv_kernel, conv_norm_gain,
    conv_norm_shift, short_kernel, recur_map, input_map, decay_param, decay_shift, initial_state, conv_out_w,
    rnn_out_w,
):
    n = lax.axis_size("sp")
    m = lax.axis_size("tp")
    f32, bf16 = jnp.float32, jnp.bfloat16
    quarter, model = tokens.shape
    depth, ca = conv_value_w.shape
    cr = rnn_input_w.shape[1]
    wid = conv_out_w.shape[1]
    heads = recur_map.shape[0]
    taps, short = conv_kernel.shape[0], short_kernel.shape[0]
    length = quarter * m
    tiles = length // 128
    pad = -(-(taps - 1) // 8) * 8
    wide = max(ca, cr)
    pack_rows = -(-(short + 4) // 8) * 8
    vmem = pl.BlockSpec(memory_space=pltpu.VMEM)
    anyw = pl.BlockSpec(memory_space=pl.ANY)
    na, nu = n // 2, m // 2
    dma = pltpu.SemaphoreType.DMA
    dims = (depth, quarter, ca, cr, wid, heads, taps, short)
    return pl.pallas_call(
        functools.partial(fused_kernel, n, m, dims),
        out_shape=jax.ShapeDtypeStruct((quarter, model), bf16),
        in_specs=[anyw] * 17,
        out_specs=vmem,
        scratch_shapes=[
            pltpu.VMEM((quarter, model), bf16),
            pltpu.VMEM((model,), bf16),
            pltpu.VMEM((quarter, model), bf16),
            pltpu.VMEM((m, quarter, model), bf16),
            pltpu.VMEM((n, depth, 2 * ca), bf16),
            pltpu.VMEM((n, depth, cr), bf16),
            pltpu.VMEM((n, depth, cr), bf16),
            pltpu.VMEM((2, na, 2, ca + cr, wid // 2), bf16),
            pltpu.VMEM(conv_kernel.shape, bf16),
            pltpu.VMEM((ca,), bf16),
            pltpu.VMEM((ca,), bf16),
            pltpu.VMEM(short_kernel.shape, bf16),
            pltpu.VMEM((2,) + recur_map.shape, bf16),
            pltpu.VMEM((cr,), f32),
            pltpu.VMEM((cr,), f32),
            pltpu.VMEM((pack_rows, wide), f32),
            pltpu.VMEM((-(-taps // 8) * 8, ca), f32),
            pltpu.VMEM((2, cr, cr), bf16),
            pltpu.VMEM((heads, length), f32),
            pltpu.VMEM((ca // 128, pad + length, 128), f32),
            pltpu.VMEM((ca // 128, length, 128), f32),
            pltpu.VMEM((tiles, 8, 128), f32),
            pltpu.VMEM((m - 1, tiles, 8, 128), f32),
            pltpu.VMEM((cr // 128, 8 + length, 128), f32),
            pltpu.VMEM((length, cr), bf16),
            pltpu.VMEM((length, cr), f32),
            pltpu.VMEM((length, cr), f32),
            pltpu.VMEM((length, 128), f32),
            pltpu.VMEM((length, cr), bf16),
            pltpu.VMEM((length, ca), bf16),
            pltpu.VMEM((length, cr), bf16),
            pltpu.VMEM((8, cr), f32),
            pltpu.VMEM((n, 8, cr), f32),
            pltpu.VMEM((2, na, m, quarter, wid), bf16),
            pltpu.VMEM((m, 2, na, quarter, wid), bf16),
            dma((2,)), dma((8,)), dma((8,)), dma((9,)), dma((9,)),
            dma((5, 2, na)), dma((5, na)), dma((5, na)), dma((5, na)),
            dma((2,)), dma((2,)), dma((max(nu - 1, 1), 2)), dma((max(nu - 1, 1), 2)),
            dma((2,)), dma((2,)), dma((m - 1,)), dma((m - 1,)),
            dma((n - 1,)), dma((n - 1,)), dma((2, na, m)), dma((2, na, m)),
        ],
        cost_estimate=pl.CostEstimate(
            flops=2 * length * (model * 2 * (ca + cr) + (ca + cr) * model), bytes_accessed=10_000_000,
            transcendentals=0,
        ),
        compiler_params=pltpu.CompilerParams(
            collective_id=7, has_side_effects=True, vmem_limit_bytes=60 * 1024 * 1024
        ),
    )(
        tokens, norm_gain, conv_value_w, conv_gate_w, rnn_input_w, rnn_gate_w, conv_out_w, rnn_out_w,
        conv_kernel, conv_norm_gain, conv_norm_shift, short_kernel, recur_map, input_map, decay_param, initial_state,
        decay_shift.T,
    )


def fits(n, m, args):
    quarter, model = args[0].shape
    depth, ca = args[2].shape
    cr = args[4].shape[1]
    wid = args[15].shape[1]
    heads = args[10].shape[0]
    return (
        n == 8 and m % 2 == 0 and wid % 256 == 0 and ca % 256 == 0 and cr % 128 == 0 and depth % 16 == 0
        and quarter % 32 == 0 and (quarter * m) % 256 == 0 and heads <= 8
    )


def whole_program(*args):
    n = lax.axis_size("sp")
    m = lax.axis_size("tp")
    return fused(*args) if fits(n, m, args) else local(*args)


def solution(mesh):
    return jax.shard_map(
        whole_program,
        mesh=mesh,
        in_specs=(
            P(("sp", "tp"), None),
            P(),
            P("sp", "tp"),
            P("sp", "tp"),
            P("sp", "tp"),
            P("sp", "tp"),
            P(None, "tp"),
            P("tp"),
            P("tp"),
            P(None, "tp"),
            P("tp", None, None),
            P("tp", None, None),
            P("tp"),
            P("sp", "tp"),
            P("tp"),
            P("tp", "sp"),
            P("tp", "sp"),
        ),
        out_specs=P(("sp", "tp"), None),
        check_vma=False,
    )
```

```python
import functools

import jax
import jax.numpy as jnp
from jax import lax
from jax.experimental import pallas as pl
from jax.experimental.pallas import tpu as pltpu
from jax.sharding import PartitionSpec as P

EPS = 1e-06
EXPONENT = 8.0


def shifted(x, axis, by):
    peers = lax.axis_size(axis)
    pairs = [(i, i + by) for i in range(peers) if 0 <= i + by < peers]
    return lax.ppermute(x, axis, pairs)


def send_to(src, dst, send, recv, axis, peer):
    return pltpu.make_async_remote_copy(
        src_ref=src,
        dst_ref=dst,
        send_sem=send,
        recv_sem=recv,
        device_id={axis: peer},
        device_id_type=pl.DeviceIdType.MESH,
    )


def project_kernel(n, m, x_ref, w_ref, o_ref, blocks, piece, acc, ring_send, ring_recv, tok_send, tok_recv, own_sem):
    half = n // 2
    me = lax.axis_index("sp")
    lane = lax.axis_index("tp")
    at = jnp.where(me % 2 == 0, me // 2, n - 1 - me // 2)

    def device_at(place):
        place = lax.rem(place + 2 * n, n)
        return jnp.where(place < half, 2 * place, 2 * (n - 1 - place) + 1)

    right = device_at(at + 1)
    left = device_at(at - 1)
    barrier = pltpu.get_barrier_semaphore()
    for peer in (left, right):
        pl.semaphore_signal(barrier, inc=1, device_id={"sp": peer}, device_id_type=pl.DeviceIdType.MESH)
    for i in range(1, m):
        pl.semaphore_signal(
            barrier, inc=1, device_id={"tp": lax.rem(lane + i, m)}, device_id_type=pl.DeviceIdType.MESH
        )
    own_w = pltpu.make_async_copy(w_ref, blocks.at[me], own_sem.at[0])
    own_x = pltpu.make_async_copy(x_ref, piece.at[lane], own_sem.at[1])
    own_w.start()
    own_x.start()
    own_w.wait()
    own_x.wait()
    pl.semaphore_wait(barrier, 2 + m - 1)
    rows = w_ref.shape[0] // 2

    def hop(way, k, part=None):
        slot = device_at(at - (k - 1)) if way == 0 else device_at(at + (k - 1))
        ref = blocks.at[slot] if part is None else blocks.at[slot, pl.ds(part * rows, rows)]
        return send_to(
            ref, ref, ring_send.at[way, k - 1], ring_recv.at[way, k - 1], "sp", right if way == 0 else left
        )

    tokens_out = [
        send_to(x_ref, piece.at[lane], tok_send.at[i - 1], tok_recv.at[i - 1], "tp", lax.rem(lane + i, m))
        for i in range(1, m)
    ]

    def add(slot, first=False):
        def one(j, _):
            here = pl.ds(pl.multiple_of(j * piece.shape[2], piece.shape[2]), piece.shape[2])
            term = jnp.dot(piece[j, slot], blocks[slot], preferred_element_type=jnp.float32)
            acc[here, :] = term if first else acc[here, :] + term
            return 0

        lax.fori_loop(0, m, one, 0)

    hop(0, 1).start()
    hop(1, 1).start()
    for copy in tokens_out:
        copy.start()
    hop(0, 1).wait_recv()
    hop(1, 1).wait_recv()
    hop(0, 2).start()
    hop(1, 2).start()
    for copy in tokens_out:
        copy.wait_recv()
    add(me, True)

    def step(k, _):
        add(device_at(at - (k - 1)))
        add(device_at(at + (k - 1)))
        hop(0, k).wait_recv()
        hop(1, k).wait_recv()

        @pl.when(k + 1 < half)
        def _():
            hop(0, k + 1).start()
            hop(1, k + 1).start()

        return 0

    lax.fori_loop(2, half, step, 0)
    hop(0, half, 0).start()
    hop(1, half, 1).start()
    add(device_at(at - (half - 1)))
    add(device_at(at + (half - 1)))
    hop(0, half, 0).wait_recv()
    hop(1, half, 1).wait_recv()
    add(device_at(at + half))

    def finish(j, _):
        here = pl.ds(pl.multiple_of(j * piece.shape[2], piece.shape[2]), piece.shape[2])
        o_ref[here, :] = acc[here, :].astype(o_ref.dtype)
        return 0

    lax.fori_loop(0, m, finish, 0)

    def sent(k, _):
        hop(0, k).wait_send()
        hop(1, k).wait_send()
        return 0

    lax.fori_loop(1, half, sent, 0)
    hop(0, half, 0).wait_send()
    hop(1, half, 1).wait_send()
    for copy in tokens_out:
        copy.wait_send()


def project(normed, weight):
    n = lax.axis_size("sp")
    m = lax.axis_size("tp")
    rows = normed.shape[0]
    depth, columns = weight.shape
    sliced = normed.reshape(rows, n, depth).transpose(1, 0, 2)
    vmem = pl.BlockSpec(memory_space=pltpu.VMEM)
    return pl.pallas_call(
        functools.partial(project_kernel, n, m),
        out_shape=jax.ShapeDtypeStruct((rows * m, columns), jnp.bfloat16),
        in_specs=[vmem, vmem],
        out_specs=vmem,
        scratch_shapes=[
            pltpu.VMEM((n, depth, columns), jnp.bfloat16),
            pltpu.VMEM((m, n, rows, depth), jnp.bfloat16),
            pltpu.VMEM((rows * m, columns), jnp.float32),
            pltpu.SemaphoreType.DMA((2, n // 2)),
            pltpu.SemaphoreType.DMA((2, n // 2)),
            pltpu.SemaphoreType.DMA((m - 1,)),
            pltpu.SemaphoreType.DMA((m - 1,)),
            pltpu.SemaphoreType.DMA((2,)),
        ],
        cost_estimate=pl.CostEstimate(
            flops=2 * rows * m * depth * n * columns, bytes_accessed=90_000_000, transcendentals=0
        ),
        compiler_params=pltpu.CompilerParams(
            collective_id=0, has_side_effects=True, vmem_limit_bytes=50 * 1024 * 1024
        ),
    )(sliced, weight)


def spread_kernel(n, axis, x_ref, o_ref, send, recv):
    me = lax.axis_index(axis)
    barrier = pltpu.get_barrier_semaphore()

    def greet(i, _):
        pl.semaphore_signal(
            barrier, inc=1, device_id={axis: lax.rem(me + i, n)}, device_id_type=pl.DeviceIdType.MESH
        )
        return 0

    lax.fori_loop(1, n, greet, 0)
    pl.semaphore_wait(barrier, n - 1)

    def copy(i):
        return send_to(x_ref, o_ref.at[me], send.at[i - 1], recv.at[i - 1], axis, lax.rem(me + i, n))

    def start(i, _):
        copy(i).start()
        return 0

    def wait(i, _):
        copy(i).wait()
        return 0

    lax.fori_loop(1, n, start, 0)
    o_ref[pl.ds(me, 1)] = x_ref[...][None]
    lax.fori_loop(1, n, wait, 0)


def spread_over(x, axis, collective_id):
    n = lax.axis_size(axis)
    vmem = pl.BlockSpec(memory_space=pltpu.VMEM)
    return pl.pallas_call(
        functools.partial(spread_kernel, n, axis),
        out_shape=jax.ShapeDtypeStruct((n,) + x.shape, x.dtype),
        in_specs=[vmem],
        out_specs=vmem,
        scratch_shapes=[pltpu.SemaphoreType.DMA((n - 1,)), pltpu.SemaphoreType.DMA((n - 1,))],
        cost_estimate=pl.CostEstimate(flops=0, bytes_accessed=10_000_000, transcendentals=0),
        compiler_params=pltpu.CompilerParams(
            collective_id=collective_id, has_side_effects=True, vmem_limit_bytes=4 * 1024 * 1024
        ),
    )(x)


def scan_kernel(parts, a_ref, b_ref, p_ref, h_ref):
    length, width = a_ref.shape
    run = length // parts
    cols = [slice(None)]

    def one(i, state):
        place = pl.ds(i, parts, stride=run)
        new = []
        for c, (p, h) in zip(cols, state):
            a = a_ref[place, c]
            h = a * h + b_ref[place, c]
            p = a * p
            p_ref[place, c] = p
            h_ref[place, c] = h
            new.append((p, h))
        return new

    first = [(jnp.ones((parts, width), jnp.float32), jnp.zeros((parts, width), jnp.float32)) for _ in cols]
    ends = lax.fori_loop(0, run, one, first)
    for c, (p, h) in zip(cols, ends):
        carry_p = p[0:1]
        carry_h = h[0:1]
        for s in range(1, parts):
            here = pl.ds(s * run, run)
            local_p = p_ref[here, c]
            h_ref[here, c] = h_ref[here, c] + local_p * carry_h
            p_ref[here, c] = local_p * carry_p
            carry_h = p[s : s + 1] * carry_h + h[s : s + 1]
            carry_p = p[s : s + 1] * carry_p


def scan(a, b):
    block = pl.BlockSpec((a.shape[0], 128), lambda c: (0, c))
    return pl.pallas_call(
        functools.partial(scan_kernel, 8),
        grid=(a.shape[1] // 128,),
        out_shape=[jax.ShapeDtypeStruct(a.shape, jnp.float32)] * 2,
        in_specs=[block, block],
        out_specs=[block, block],
        cost_estimate=pl.CostEstimate(flops=4 * a.size, bytes_accessed=16 * a.size, transcendentals=0),
        compiler_params=pltpu.CompilerParams(vmem_limit_bytes=20 * 1024 * 1024),
    )(a, b)


def entering(last_decay, last_drive, initial):
    n = lax.axis_size("sp")
    place = lax.axis_index("sp")
    pair = jnp.stack([last_decay, last_drive])
    gathered = spread_over(jnp.pad(pair, ((0, 6), (0, 0))), "sp", 1)
    state = initial
    for i in range(n):
        state = jnp.where(i < place, gathered[i, 0] * state + gathered[i, 1], state)
    return state


def causal_taps(extended, kernel, length):
    result = jnp.zeros((length, extended.shape[1]), jnp.float32)
    for offset in range(kernel.shape[0]):
        result = result + kernel[offset].astype(jnp.float32) * extended[offset : offset + length]
    return result


def block_diagonal(values, maps):
    heads, size, _ = maps.shape
    rows = [
        jnp.pad(maps[h], ((0, 0), (h * size, (heads - 1 - h) * size))) for h in range(heads)
    ]
    return jnp.dot(values, jnp.concatenate(rows, axis=0), preferred_element_type=jnp.float32)


def local(
    tokens,
    norm_gain,
    conv_value_w,
    conv_gate_w,
    rnn_input_w,
    rnn_gate_w,
    conv_kernel,
    conv_norm_gain,
    conv_norm_shift,
    short_kernel,
    recur_map,
    input_map,
    decay_param,
    decay_shift,
    initial_state,
    conv_out_w,
    rnn_out_w,
):
    as_float = tokens.astype(jnp.float32)
    scale = lax.rsqrt(jnp.mean(as_float * as_float, axis=1, keepdims=True) + EPS)
    normed = (as_float * scale * norm_gain.astype(jnp.float32)).astype(jnp.bfloat16)
    edges = [0]
    for weight in (conv_value_w, conv_gate_w, rnn_input_w, rnn_gate_w):
        edges.append(edges[-1] + weight.shape[1])
    joined = project(
        normed, jnp.concatenate([conv_value_w, conv_gate_w, rnn_input_w, rnn_gate_w], axis=1)
    )
    conv_value, conv_gate, rnn_input, rnn_gate = [
        joined[:, edges[index] : edges[index + 1]] for index in range(4)
    ]
    out_weights = (
        lax.all_gather(conv_out_w, "sp", axis=1, tiled=True),
        lax.all_gather(rnn_out_w, "sp", axis=1, tiled=True),
    )
    length = conv_value.shape[0]
    conv_reach = conv_kernel.shape[0] - 1
    short_reach = short_kernel.shape[0] - 1
    tail = shifted(joined[length - conv_reach :, : edges[3]], "sp", 1)
    value_tail = tail[:, : edges[1]]
    gate_tail = tail[:, edges[1] : edges[2]]
    input_tail = tail[conv_reach - short_reach :, edges[2] :]
    value_ext = jnp.concatenate([value_tail, conv_value], axis=0)
    gate_ext = jnp.concatenate([gate_tail, conv_gate], axis=0)
    input_ext = jnp.concatenate([input_tail, rnn_input], axis=0)
    gated_values = value_ext.astype(jnp.float32) * jax.nn.sigmoid(gate_ext.astype(jnp.float32))
    conv_mixed = causal_taps(gated_values, conv_kernel, length)
    moments = lax.psum(
        (jnp.sum(conv_mixed, axis=1), jnp.sum(conv_mixed * conv_mixed, axis=1)), "tp"
    )
    channels = conv_mixed.shape[1] * lax.axis_size("tp")
    average = moments[0][:, None] / channels
    spread = moments[1][:, None] / channels - average * average
    scaled = (conv_mixed - average) * lax.rsqrt(spread + EPS)
    scaled = scaled * conv_norm_gain.astype(jnp.float32) + conv_norm_shift.astype(jnp.float32)
    conv_hidden = jax.nn.silu(scaled).astype(jnp.bfloat16)
    rnn_short = causal_taps(input_ext.astype(jnp.float32), short_kernel, length).astype(
        jnp.bfloat16
    )
    recur_gate = jax.nn.sigmoid(block_diagonal(rnn_short, recur_map))
    input_gate = jax.nn.sigmoid(block_diagonal(rnn_short, input_map))
    shift_cols = jnp.repeat(decay_shift, recur_map.shape[1], axis=1)
    log_decay = -EXPONENT * recur_gate * jax.nn.softplus(-decay_param)[None, :] + shift_cols
    drive = jnp.sqrt(-jnp.expm1(2.0 * log_decay)) * input_gate * rnn_short.astype(jnp.float32)
    cum_decay, cum_drive = scan(jnp.exp(log_decay), drive)
    state_before = entering(cum_decay[length - 1], cum_drive[length - 1], initial_state)
    states = cum_drive + cum_decay * state_before[None, :]
    rnn_hidden = (states * jax.nn.gelu(rnn_gate.astype(jnp.float32), approximate=True)).astype(
        jnp.bfloat16
    )
    return lax.psum_scatter(
        (
            jnp.dot(conv_hidden, out_weights[0], preferred_element_type=jnp.float32)
            + jnp.dot(rnn_hidden, out_weights[1], preferred_element_type=jnp.float32)
        ).astype(jnp.bfloat16),
        "tp",
        scatter_dimension=0,
        tiled=True,
    )


def fused_kernel(n, m, dims, *refs):
    depth, quarter, ca, cr, wid, heads, taps, short = dims
    (
        tok_ref, ngain_hbm, wv_ref, wg_ref, wri_ref, wrg_ref, wco_ref, wro_ref, taps_hbm, cgain_hbm, cshift_hbm,
        short_hbm, rmap_hbm, imap_hbm, decay_hbm, init_hbm, sh_hbm,
        o_ref,
        TB, NGB, NB, X, BC, BI, BG, BO, KB, CGB, CSB, SKB, RM, DPB, ISB, PK, PC, BD, SH, G, MIX, MS, MR, E, S, Z0, Z1, SHC, RG, HC, HR, SM, SR, PB, R,
        own_sem, swap_send, swap_recv, par_send, par_recv, line_send, line_recv, sib_send, sib_recv,
        tok_send, tok_recv, tokf_send, tokf_recv, halo_send, halo_recv, mom_send, mom_recv,
        state_send, state_recv, rs_send, rs_recv,
    ) = refs
    f32, bf16 = jnp.float32, jnp.bfloat16
    na, nu = n // 2, m // 2
    length = quarter * m
    model = depth * n
    half = length // 2
    reach = taps - 1
    pad = -(-reach // 8) * 8
    lanes = 128
    ga, gr = ca // lanes, cr // lanes
    tiles = length // lanes
    sp = lax.axis_index("sp")
    tp = lax.axis_index("tp")
    a, b = sp // 2, sp % 2
    u, v = tp // 2, tp % 2
    same = b == v
    other = b != v
    spc = 2 * a + v
    tpc = 2 * u + b

    def at(s, t):
        return {"sp": s, "tp": t}

    def where_is(s, t):
        return at(2 * (s // 2) + t % 2, 2 * (t // 2) + s % 2)

    partner = at(2 * a + v, 2 * u + b)
    sibling = at(sp, 2 * u + 1 - v)

    def remote(src, dst, send, recv, dev):
        return pltpu.make_async_remote_copy(
            src_ref=src, dst_ref=dst, send_sem=send, recv_sem=recv, device_id=dev,
            device_id_type=pl.DeviceIdType.MESH,
        )

    barrier = pltpu.get_barrier_semaphore()
    gets = [
        pltpu.make_async_copy(tok_ref, TB, own_sem.at[0]),
        pltpu.make_async_copy(ngain_hbm, NGB, own_sem.at[1]),
    ]
    for get in gets:
        get.start()
    for i in range(n):
        s_ = sp + i
        s_ = jnp.where(s_ >= n, s_ - n, s_)
        for j in range(m):
            if i or j:
                t_ = tp + j
                t_ = jnp.where(t_ >= m, t_ - m, t_)
                pl.semaphore_signal(barrier, inc=1, device_id=at(s_, t_), device_id_type=pl.DeviceIdType.MESH)

    hw = wid // 2
    bufs = [
        lambda o, core: BC.at[2 * o + core],
        lambda o, core: BI.at[2 * o + core],
        lambda o, core: BG.at[2 * o + core],
        lambda o, core: BO.at[0, o, core],
        lambda o, core: BO.at[1, o, core],
    ]
    parts = [
        [(wv_ref, lambda j: BC.at[j, :, pl.ds(0, ca)]), (wg_ref, lambda j: BC.at[j, :, pl.ds(ca, ca)])],
        [(wri_ref, lambda j: BI.at[j])],
        [(wrg_ref, lambda j: BG.at[j])],
    ]
    for e in range(2):
        here = pl.ds(e * hw, hw)
        parts.append([
            (wco_ref.at[:, here], lambda j, e=e: BO.at[e, j // 2, j % 2, pl.ds(0, ca)]),
            (wro_ref.at[:, here], lambda j, e=e: BO.at[e, j // 2, j % 2, pl.ds(ca, cr)]),
        ])
    first = [0, 2, 3, 4, 6]

    def each_part(s, act):
        for p, (src, dst) in enumerate(parts[s]):
            act(src, dst, first[s] + p)

    def bring_local(s):
        each_part(s, lambda src, dst, k: pltpu.make_async_copy(src, dst(spc), swap_recv.at[k]).start())

    def swapped(src, dst, k):
        return remote(src, dst(sp), swap_send.at[k], swap_recv.at[k], partner)

    def bring_remote(s):
        each_part(s, lambda src, dst, k: swapped(src, dst, k).start())

    def brought(s):
        @pl.when(same)
        def _():
            each_part(s, lambda src, dst, k: pltpu.make_async_copy(src, dst(spc), swap_recv.at[k]).wait())

        @pl.when(other)
        def _():
            each_part(s, lambda src, dst, k: swapped(src, dst, k).wait_recv())

    params = [
        (taps_hbm, KB), (cgain_hbm, CGB), (cshift_hbm, CSB), (short_hbm, SKB), (decay_hbm, DPB), (init_hbm, ISB),
        (rmap_hbm, RM.at[0]), (imap_hbm, RM.at[1]),
    ]
    np_ = len(params)

    @pl.when(same)
    def _():
        for s in range(5):
            bring_local(s)
        for k, (src, dst) in enumerate(params):
            pltpu.make_async_copy(src, dst, par_recv.at[k]).start()
        pltpu.make_async_copy(sh_hbm, SH, par_recv.at[np_]).start()

    pl.semaphore_wait(barrier, n * m - 1)

    def param_send(k):
        return remote(params[k][0], params[k][1], par_send.at[k], par_recv.at[k], sibling)

    shift_send = remote(sh_hbm, SH, par_send.at[np_], par_recv.at[np_], partner)

    tok_peer = remote(NB, X.at[tp], tok_send.at[0], tok_recv.at[v], at(2 * a + 1 - b, 2 * u + b))
    tok_sib = remote(NB, X.at[tp], tok_send.at[1], tok_recv.at[v], sibling)

    @pl.when(other)
    def _():
        bring_remote(0)

    def block(s, o, core):
        return bufs[s](o, core) if isinstance(s, int) else BO.at[s - 3, o, core]

    def up(s, o):
        ref = block(s, o, v)
        return remote(ref, ref, line_send.at[s, 0, o], line_recv.at[s, o], at(2 * a + 2 + b, tp))

    def down(s, o):
        ref = block(s, o, v)
        return remote(ref, ref, line_send.at[s, 1, o], line_recv.at[s, o], at(2 * a - 2 + b, tp))

    def across(s, o, core):
        ref = block(s, o, core)
        return remote(ref, ref, sib_send.at[s, o], sib_recv.at[s, o], sibling)

    low = a < na // 2

    def inward(s, k, act):
        @pl.when(jnp.logical_and(low, a - k >= 0))
        def _():
            act(up(s, a - k))

        @pl.when(jnp.logical_and(jnp.logical_not(low), a + k < na))
        def _():
            act(down(s, a + k))

    def outward(s, k, act):
        @pl.when(jnp.logical_and(jnp.logical_and(low, a > 0), a + k < na))
        def _():
            act(down(s, a + k))

        @pl.when(jnp.logical_and(jnp.logical_and(jnp.logical_not(low), a + 1 < na), a - k >= 0))
        def _():
            act(up(s, a - k))

    window = 2
    going_in, going_out = [], []

    def push(way, order, s, k):
        if len(order) >= window:
            way(*order[-window], lambda c: c.wait_send())
        way(s, k, lambda c: c.start())
        order.append((s, k))

    def push_in(s, k):
        push(inward, going_in, s, k)

    def push_out(s, k):
        push(outward, going_out, s, k)

    def hold(s):
        brought(s)
        across(s, a, v).start()

    def take(s, k):
        @pl.when(a - k >= 0)
        def _():
            up(s, a - k).wait_recv()
            across(s, a - k, v).start()

        @pl.when(a + k < na)
        def _():
            down(s, a + k).wait_recv()
            across(s, a + k, v).start()

    def crossed(s):
        def one(o, _):
            across(s, o, 1 - v).wait_recv()
            return 0

        lax.fori_loop(0, na, one, 0)

    def tok_from(c):
        q = 2 * u + c
        return remote(NB, X.at[q], tok_send.at[0], tok_recv.at[c], sibling)

    def tok_forward(i, uu, c):
        ref = X.at[2 * uu + c]
        return remote(ref, ref, tokf_send.at[i - 1, c], tokf_recv.at[i - 1, c], at(sp, 2 * ((u + i) % nu) + v))

    at_end = jnp.logical_or(a == 0, a == na - 1)

    def mids(f):
        return pl.when(jnp.logical_not(at_end))(f)

    def ends(f):
        return pl.when(at_end)(f)

    def token_relay(c):
        @pl.when(jnp.logical_or(other, v != c))
        def _():
            tok_from(c).wait_recv()

        for i in range(1, nu):
            tok_forward(i, u, c).start()

    def first_sends():
        brought(0)
        across(0, a, v).start()
        inward(0, 0, lambda c: c.start())
        outward(0, 0, lambda c: c.start())

    @pl.when(same)
    def _():
        first_sends()

    for get in gets:
        get.wait()
    gain = NGB[...].astype(f32).reshape(1, model)

    def norm(i, _):
        rows = pl.ds(pl.multiple_of(i * 32, 32), 32)
        t = TB[rows, :].astype(f32)
        scale = lax.rsqrt(jnp.sum(t * t, axis=1, keepdims=True) * (1.0 / model) + EPS)
        y = (t * scale * gain).astype(bf16)
        NB[rows, :] = y

        @pl.when(same)
        def _():
            X[tp, rows, :] = y

        return 0

    lax.fori_loop(0, quarter // 32, norm, 0)
    @pl.when(same)
    def _():
        tok_peer.start()
        for k in range(np_):
            param_send(k).start()

    going_in.append((0, 0))
    going_out.append((0, 0))

    @pl.when(other)
    def _():
        first_sends()
        bring_remote(1)
        tok_sib.start()
        tok_peer.start()

    hold(1)
    push_in(1, 0)
    push_out(1, 0)
    take(0, 1)
    push_in(0, 1)
    push_out(0, 1)
    token_relay(v)
    take(1, 1)
    push_in(1, 1)
    push_out(1, 1)
    token_relay(1 - v)

    @pl.when(other)
    def _():
        bring_remote(2)
        shift_send.start()
        bring_remote(3)
        bring_remote(4)

    take(0, 2)
    push_out(0, 2)

    @mids
    def _():
        take(1, 2)
        push_out(1, 2)

    hold(2)
    push_in(2, 0)

    @pl.when(same)
    def _():
        for k, (src, dst) in enumerate(params):
            pltpu.make_async_copy(src, dst, par_recv.at[k]).wait()
        pltpu.make_async_copy(sh_hbm, SH, par_recv.at[np_]).wait()

    @pl.when(other)
    def _():
        for k in range(np_):
            param_send(k).wait_recv()
        shift_send.wait_recv()

    head = cr // heads
    PC[0:taps, :] = KB[...].astype(f32)
    PK[0:1, 0:ca] = CGB[...].astype(f32).reshape(1, ca)
    PK[1:2, 0:ca] = CSB[...].astype(f32).reshape(1, ca)
    PK[2 : 2 + short, 0:cr] = SKB[...].astype(f32)
    x = -DPB[...].reshape(1, cr)
    z = jnp.exp(-jnp.abs(x))
    z = z / (2.0 + z)
    z2 = z * z
    series = jnp.full_like(z, 1.0 / 17.0)
    for k in range(15, 0, -2):
        series = series * z2 + 1.0 / k
    PK[2 + short : 3 + short, 0:cr] = -EXPONENT * (jnp.maximum(x, 0.0) + 2.0 * z * series)
    PK[3 + short : 4 + short, 0:cr] = ISB[...].reshape(1, cr)
    for g in range(2):
        BD[g] = jnp.zeros((cr, cr), bf16)
        for h in range(heads):
            BD[g, h * head : (h + 1) * head, h * head : (h + 1) * head] = RM[g, h]

    def shift_columns(i, _):
        cols = SH[:, pl.ds(pl.multiple_of(i * lanes, lanes), lanes)]
        full = jnp.concatenate([cols, jnp.zeros((lanes - heads, lanes), f32)], axis=0)
        SHC[pl.ds(pl.multiple_of(i * lanes, lanes), lanes), :] = full.T
        return 0

    lax.fori_loop(0, tiles, shift_columns, 0)

    @ends
    def _():
        take(0, 3)

    for i in range(1, nu):
        for c in range(2):
            tok_forward(i, (u - i + nu) % nu, c).wait_recv()
    crossed(0)

    chunk = 256
    cols_a = ca // chunk

    def tokens_half(r):
        return X[pl.ds(r * nu, nu)].reshape(half, model)

    def conv_project(i, _):
        r, j = i // cols_a, i % cols_a
        x = tokens_half(r)
        at_v = pl.ds(pl.multiple_of(j * chunk, chunk), chunk)
        at_g = pl.ds(pl.multiple_of(ca + j * chunk, chunk), chunk)
        val = jnp.dot(x, BC[:, :, at_v].reshape(model, chunk), preferred_element_type=f32).astype(bf16)
        gate = jnp.dot(x, BC[:, :, at_g].reshape(model, chunk), preferred_element_type=f32).astype(bf16)
        out = val.astype(f32) * jax.nn.sigmoid(gate.astype(f32))
        rows = pl.ds(pl.multiple_of(pad + r * half, 8), half)
        for g in range(chunk // lanes):
            G[j * (chunk // lanes) + g, rows, :] = out[:, g * lanes : (g + 1) * lanes]
        return 0

    lax.fori_loop(0, 2 * cols_a, conv_project, 0)
    behind = where_is(spc + 1, tpc)
    conv_halo = remote(
        G.at[:, pl.ds(length, pad)], G.at[:, pl.ds(0, pad)], halo_send.at[0], halo_recv.at[0], behind
    )
    rnn_halo = remote(
        E.at[:, pl.ds(length, 8)], E.at[:, pl.ds(0, 8)], halo_send.at[1], halo_recv.at[1], behind
    )

    @pl.when(spc + 1 < n)
    def _():
        conv_halo.start()

    @mids
    def _():
        push_out(2, 0)
        take(2, 1)

    push_in(2, 1)
    hold(3)
    push_in(3, 0)
    hold(4)
    push_in(4, 0)

    @pl.when(spc == 0)
    def _():
        G[:, 0:pad, :] = jnp.zeros((ga, pad, lanes), f32)
        E[:, 0:8, :] = jnp.zeros((gr, 8, lanes), f32)

    @pl.when(spc > 0)
    def _():
        conv_halo.wait_recv()

    @mids
    def _():
        push_out(2, 1)

    lane = lax.broadcasted_iota(jnp.int32, (lanes, lanes), 1)
    sub = lax.broadcasted_iota(jnp.int32, (lanes, lanes), 0)

    def convolve(i, _):
        t0 = pl.multiple_of(i * lanes, lanes)
        sums = jnp.zeros((lanes, lanes), f32)
        squares = jnp.zeros((lanes, lanes), f32)
        for g in range(ga):
            here = slice(g * lanes, (g + 1) * lanes)
            acc = jnp.zeros((lanes, lanes), f32)
            for k in range(taps):
                acc = acc + PC[k : k + 1, here] * G[g, pl.ds(t0 + (pad - reach + k), lanes), :]
            MIX[g, pl.ds(t0, lanes), :] = acc
            sums = sums + acc
            squares = squares + acc * acc
        s1 = jnp.sum(sums, axis=1, keepdims=True)
        s2 = jnp.sum(squares, axis=1, keepdims=True)
        both = jnp.where(lane == 0, s1, jnp.where(lane == 1, s2, 0.0))
        MS[i] = both.T[0:8, :]
        return 0

    lax.fori_loop(0, tiles, convolve, 0)

    def moments(i):
        return remote(
            MS, MR.at[i - 1], mom_send.at[i - 1], mom_recv.at[i - 1], where_is(spc, (tpc + i) % m)
        )

    for i in range(1, m):
        moments(i).start()

    @mids
    def _():
        take(2, 2)
        push_out(2, 2)

    @ends
    def _():
        take(1, 2)
        take(1, 3)

    crossed(1)

    spans = []
    left = 0
    while left < cr:
        spans.append((left, min(chunk, cr - left)))
        left += chunk

    def input_project(r, _):
        x = tokens_half(r)
        rows = pl.ds(pl.multiple_of(8 + r * half, 8), half)
        for lo, size in spans:
            out = jnp.dot(x, BI[:, :, lo : lo + size].reshape(model, size), preferred_element_type=f32)
            out = out.astype(bf16).astype(f32)
            for g in range(size // lanes):
                E[lo // lanes + g, rows, :] = out[:, g * lanes : (g + 1) * lanes]
        return 0

    lax.fori_loop(0, 2, input_project, 0)

    @pl.when(spc + 1 < n)
    def _():
        rnn_halo.start()

    @pl.when(spc > 0)
    def _():
        rnn_halo.wait_recv()

    def short_conv(i, _):
        t0 = pl.multiple_of(i * lanes, lanes)
        for g in range(gr):
            here = slice(g * lanes, (g + 1) * lanes)
            acc = jnp.zeros((lanes, lanes), f32)
            for k in range(short):
                acc = acc + PK[2 + k : 3 + k, here] * E[g, pl.ds(t0 + (8 - short + 1 + k), lanes), :]
            S[pl.ds(t0, lanes), here] = acc.astype(bf16)
        return 0

    lax.fori_loop(0, tiles, short_conv, 0)

    def gate_maps(r, _):
        rows = pl.ds(pl.multiple_of(r * half, half), half)
        s = S[rows, :]
        Z0[rows, :] = jnp.dot(s, BD[0], preferred_element_type=f32)
        Z1[rows, :] = jnp.dot(s, BD[1], preferred_element_type=f32)
        return 0

    lax.fori_loop(0, 2, gate_maps, 0)

    @mids
    def _():
        take(3, 1)
        push_out(3, 0)

    push_in(3, 1)

    size = 32
    subs = size // 8
    lane32 = lax.broadcasted_iota(jnp.int32, (size, lanes), 1)
    row8 = lax.broadcasted_iota(jnp.int32, (subs, 8, lanes), 1)

    def recur(i, carry):
        rows = pl.ds(pl.multiple_of(i * size, size), size)
        shc = SHC[rows, :]
        new = []
        for g in range(gr):
            here = slice(g * lanes, (g + 1) * lanes)
            shift = None
            for h in reversed(range((g * lanes) // head, (g * lanes + lanes - 1) // head + 1)):
                col = jnp.broadcast_to(shc[:, h : h + 1], (size, lanes))
                shift = col if shift is None else jnp.where(lane32 < (h + 1) * head - g * lanes, col, shift)
            log_decay = PK[2 + short : 3 + short, here] * jax.nn.sigmoid(Z0[rows, here]) + shift
            t = jnp.tanh(log_decay)
            drive = jnp.sqrt((-2.0 * t) / (1.0 - t)) * jax.nn.sigmoid(Z1[rows, here])
            drive = drive * S[rows, here].astype(f32)
            p = jnp.exp(log_decay).reshape(subs, 8, lanes)
            h_ = drive.reshape(subs, 8, lanes)
            for d in (1, 2, 4):
                keep = row8 >= d
                ps = jnp.where(keep, pltpu.roll(p, d, 1), 1.0)
                hs = jnp.where(keep, pltpu.roll(h_, d, 1), 0.0)
                h_ = p * hs + h_
                p = p * ps
            Z0[rows, here] = p.reshape(size, lanes)
            Z1[rows, here] = h_.reshape(size, lanes)
            pc, hc = carry[g]
            for q in range(subs):
                pe = p[q, 7:8, :]
                hc = pe * hc + h_[q, 7:8, :]
                pc = pe * pc
            new.append((pc, hc))
        return new

    start = [(jnp.ones((1, lanes), f32), jnp.zeros((1, lanes), f32)) for _ in range(gr)]
    last = lax.fori_loop(0, length // size, recur, start)
    for g in range(gr):
        here = slice(g * lanes, (g + 1) * lanes)
        SM[0:1, here] = last[g][0]
        SM[1:2, here] = last[g][1]
    SM[2:8, :] = jnp.zeros((6, cr), f32)

    def state_to(i):
        return remote(SM, SR.at[spc], state_send.at[i - 1], state_recv.at[i - 1], where_is(spc + i, tpc))

    def state_from(i):
        return remote(SM, SR.at[spc - i], state_send.at[i - 1], state_recv.at[i - 1], where_is(spc, tpc))

    for i in range(1, n):

        @pl.when(spc + i < n)
        def _():
            state_to(i).start()


    @mids
    def _():
        take(4, 1)
        push_out(3, 1)

    push_in(4, 1)
    for i in range(1, m):
        moments(i).wait_recv()

    def conv_finish(i, _):
        tot = MS[i]
        for p in range(m - 1):
            tot = tot + MR[p, i]
        average = tot[0:1, :] * (1.0 / (ca * m))
        spread = tot[1:2, :] * (1.0 / (ca * m)) - average * average
        inv = lax.rsqrt(spread + EPS)
        full = jnp.where(sub == 0, average, jnp.where(sub == 1, inv, 0.0)).T
        rows = pl.ds(pl.multiple_of(i * lanes, lanes), lanes)
        av, iv = full[:, 0:1], full[:, 1:2]
        for g in range(ga):
            here = slice(g * lanes, (g + 1) * lanes)
            y = (MIX[g, rows, :] - av) * iv * PK[0:1, here] + PK[1:2, here]
            HC[rows, here] = (y * jax.nn.sigmoid(y)).astype(bf16)
        return 0

    lax.fori_loop(0, tiles, conv_finish, 0)
    @ends
    def _():
        take(2, 1)
        take(2, 2)
        take(2, 3)

    crossed(2)

    def gate_project(r, _):
        x = tokens_half(r)
        rows = pl.ds(pl.multiple_of(r * half, half), half)
        for lo, size_ in spans:
            out = jnp.dot(x, BG[:, :, lo : lo + size_].reshape(model, size_), preferred_element_type=f32)
            RG[rows, lo : lo + size_] = out.astype(bf16)
        return 0

    lax.fori_loop(0, 2, gate_project, 0)
    for i in range(1, n):

        @pl.when(spc - i >= 0)
        def _():
            state_from(i).wait_recv()

    def enter(i, state):
        return SR[i, 0:1, :] * state + SR[i, 1:2, :]

    before = lax.fori_loop(0, spc, enter, PK[3 + short : 4 + short, 0:cr])

    def rnn_finish(i, carry):
        rows = pl.ds(pl.multiple_of(i * size, size), size)
        new = []
        for g in range(gr):
            here = slice(g * lanes, (g + 1) * lanes)
            p = Z0[rows, here]
            h_ = Z1[rows, here]
            hc = carry[g]
            outs = []
            for q in range(subs):
                st = p[8 * q : 8 * q + 8] * hc + h_[8 * q : 8 * q + 8]
                outs.append(st)
                hc = st[7:8, :]
            new.append(hc)
            st = jnp.concatenate(outs, axis=0)
            gate = RG[rows, here].astype(f32)
            HR[rows, here] = (st * jax.nn.gelu(gate, approximate=True)).astype(bf16)
        return new

    lax.fori_loop(0, length // size, rnn_finish, [before[:, g * lanes : (g + 1) * lanes] for g in range(gr)])

    @mids
    def _():
        take(3, 2)
        push_out(3, 2)

    def out_copy(e, o, q):
        return remote(
            PB.at[e, o, q], R.at[tpc, e, o], rs_send.at[e, o, q], rs_recv.at[e, o, tpc], at(2 * a + v, q)
        )

    def out_from(e, o, t):
        return remote(PB.at[e, o, 0], R.at[t, e, o], rs_send.at[e, o, 0], rs_recv.at[e, o, t], sibling)

    def produce(e, o):
        across(3 + e, o, 1 - v).wait_recv()
        w = jnp.concatenate([BO[e, o, 0], BO[e, o, 1]], axis=1)
        y = jnp.dot(HC[...], w[0:ca], preferred_element_type=f32)
        y = (y + jnp.dot(HR[...], w[ca : ca + cr], preferred_element_type=f32)).astype(bf16)
        PB[e, o] = y.reshape(m, quarter, wid)
        for q in range(m):
            mine = jnp.logical_and(same, tp == q)

            @pl.when(jnp.logical_not(mine))
            def _():
                out_copy(e, o, q).start()

            @pl.when(mine)
            def _():
                R[tpc, e, o] = y[q * quarter : (q + 1) * quarter]

    def settle(e, o):
        for t in range(m):

            @pl.when(jnp.logical_or(other, tpc != t))
            def _():
                out_from(e, o, t).wait_recv()

        y = R[0, e, o].astype(f32)
        for t in range(1, m):
            y = y + R[t, e, o].astype(f32)
        y = y.astype(o_ref.dtype)
        for c in range(2):
            lo = pl.multiple_of((2 * o + c) * wid + e * hw, hw)
            o_ref[:, pl.ds(lo, hw)] = y[:, c * hw : (c + 1) * hw]

    def each_origin(i, act):
        e = jnp.where(jnp.logical_or(i == 1, i > na), 1, 0)
        k = jnp.where(i < 2, 0, jnp.where(i <= na, i - 1, i - na))

        def one(t, _):
            o = jnp.where(t == 0, a - k, a + k)
            ok = jnp.where(t == 0, o >= 0, jnp.logical_and(o < na, k > 0))

            @pl.when(ok)
            def _():
                act(e, o)

            return 0

        def ready():
            @pl.when(jnp.logical_and(at_end, k > 0))
            def _():
                take(3 + e, k)

        return ready, lambda: lax.fori_loop(0, 2, one, 0)

    def drain_early(o, _):
        for s in range(3):
            across(s, o, v).wait_send()
        return 0

    lax.fori_loop(0, na, drain_early, 0)

    @pl.when(other)
    def _():
        for s in range(5):
            each_part(s, lambda src, dst, k: swapped(src, dst, k).wait_send())
        shift_send.wait_send()
        tok_sib.wait_send()

    @pl.when(same)
    def _():
        for k in range(np_):
            param_send(k).wait_send()

    tok_peer.wait_send()
    for i in range(1, nu):
        for c in range(2):
            tok_forward(i, u, c).wait_send()

    @pl.when(spc + 1 < n)
    def _():
        conv_halo.wait_send()
        rnn_halo.wait_send()

    for i in range(1, m):
        moments(i).wait_send()
    for i in range(1, n):

        @pl.when(spc + i < n)
        def _():
            state_to(i).wait_send()

    def outer(i, _):
        ready, run = each_origin(i, produce)
        ready()

        @pl.when(jnp.logical_and(jnp.logical_not(at_end), i == na + 2))
        def _():
            take(4, 2)

        run()

        @mids
        def _():
            for stage, k in ((na - 1, 0), (na + 1, 1), (na + 2, 2)):

                @pl.when(i == stage)
                def _():
                    push_out(4, k)

        @pl.when(jnp.logical_and(at_end, i >= 3))
        def _():
            each_origin(i - 3, settle)[1]()

        return 0

    lax.fori_loop(0, 2 * na, outer, 0)

    def conclude(i, _):
        each_origin(i, settle)[1]()
        return 0

    lax.fori_loop(jnp.where(at_end, 2 * na - 3, 0), 2 * na, conclude, 0)

    def drain(o, _):
        for s in range(3, 5):
            across(s, o, v).wait_send()
        return 0

    assert len(going_in) == 10 and len(going_out) == 15
    lax.fori_loop(0, na, drain, 0)

    for way, order in ((inward, going_in), (outward, going_out)):
        for one in order[-window:]:
            way(*one, lambda c: c.wait_send())

    def drain_out(o, _):
        for e in range(2):
            for q in range(m):

                @pl.when(jnp.logical_not(jnp.logical_and(same, tp == q)))
                def _():
                    out_copy(e, o, q).wait_send()

        return 0

    lax.fori_loop(0, na, drain_out, 0)


def fused(
    tokens, norm_gain, conv_value_w, conv_gate_w, rnn_input_w, rnn_gate_w, conv_kernel, conv_norm_gain,
    conv_norm_shift, short_kernel, recur_map, input_map, decay_param, decay_shift, initial_state, conv_out_w,
    rnn_out_w,
):
    n = lax.axis_size("sp")
    m = lax.axis_size("tp")
    f32, bf16 = jnp.float32, jnp.bfloat16
    quarter, model = tokens.shape
    depth, ca = conv_value_w.shape
    cr = rnn_input_w.shape[1]
    wid = conv_out_w.shape[1]
    heads = recur_map.shape[0]
    taps, short = conv_kernel.shape[0], short_kernel.shape[0]
    length = quarter * m
    tiles = length // 128
    pad = -(-(taps - 1) // 8) * 8
    wide = max(ca, cr)
    pack_rows = -(-(short + 4) // 8) * 8
    vmem = pl.BlockSpec(memory_space=pltpu.VMEM)
    anyw = pl.BlockSpec(memory_space=pl.ANY)
    na, nu = n // 2, m // 2
    dma = pltpu.SemaphoreType.DMA
    dims = (depth, quarter, ca, cr, wid, heads, taps, short)
    return pl.pallas_call(
        functools.partial(fused_kernel, n, m, dims),
        out_shape=jax.ShapeDtypeStruct((quarter, model), bf16),
        in_specs=[anyw] * 17,
        out_specs=vmem,
        scratch_shapes=[
            pltpu.VMEM((quarter, model), bf16),
            pltpu.VMEM((model,), bf16),
            pltpu.VMEM((quarter, model), bf16),
            pltpu.VMEM((m, quarter, model), bf16),
            pltpu.VMEM((n, depth, 2 * ca), bf16),
            pltpu.VMEM((n, depth, cr), bf16),
            pltpu.VMEM((n, depth, cr), bf16),
            pltpu.VMEM((2, na, 2, ca + cr, wid // 2), bf16),
            pltpu.VMEM(conv_kernel.shape, bf16),
            pltpu.VMEM((ca,), bf16),
            pltpu.VMEM((ca,), bf16),
            pltpu.VMEM(short_kernel.shape, bf16),
            pltpu.VMEM((2,) + recur_map.shape, bf16),
            pltpu.VMEM((cr,), f32),
            pltpu.VMEM((cr,), f32),
            pltpu.VMEM((pack_rows, wide), f32),
            pltpu.VMEM((-(-taps // 8) * 8, ca), f32),
            pltpu.VMEM((2, cr, cr), bf16),
            pltpu.VMEM((heads, length), f32),
            pltpu.VMEM((ca // 128, pad + length, 128), f32),
            pltpu.VMEM((ca // 128, length, 128), f32),
            pltpu.VMEM((tiles, 8, 128), f32),
            pltpu.VMEM((m - 1, tiles, 8, 128), f32),
            pltpu.VMEM((cr // 128, 8 + length, 128), f32),
            pltpu.VMEM((length, cr), bf16),
            pltpu.VMEM((length, cr), f32),
            pltpu.VMEM((length, cr), f32),
            pltpu.VMEM((length, 128), f32),
            pltpu.VMEM((length, cr), bf16),
            pltpu.VMEM((length, ca), bf16),
            pltpu.VMEM((length, cr), bf16),
            pltpu.VMEM((8, cr), f32),
            pltpu.VMEM((n, 8, cr), f32),
            pltpu.VMEM((2, na, m, quarter, wid), bf16),
            pltpu.VMEM((m, 2, na, quarter, wid), bf16),
            dma((2,)), dma((8,)), dma((8,)), dma((9,)), dma((9,)),
            dma((5, 2, na)), dma((5, na)), dma((5, na)), dma((5, na)),
            dma((2,)), dma((2,)), dma((max(nu - 1, 1), 2)), dma((max(nu - 1, 1), 2)),
            dma((2,)), dma((2,)), dma((m - 1,)), dma((m - 1,)),
            dma((n - 1,)), dma((n - 1,)), dma((2, na, m)), dma((2, na, m)),
        ],
        cost_estimate=pl.CostEstimate(
            flops=2 * length * (model * 2 * (ca + cr) + (ca + cr) * model), bytes_accessed=10_000_000,
            transcendentals=0,
        ),
        compiler_params=pltpu.CompilerParams(
            collective_id=7, has_side_effects=True, vmem_limit_bytes=60 * 1024 * 1024
        ),
    )(
        tokens, norm_gain, conv_value_w, conv_gate_w, rnn_input_w, rnn_gate_w, conv_out_w, rnn_out_w,
        conv_kernel, conv_norm_gain, conv_norm_shift, short_kernel, recur_map, input_map, decay_param, initial_state,
        decay_shift.T,
    )


def fits(n, m, args):
    quarter, model = args[0].shape
    depth, ca = args[2].shape
    cr = args[4].shape[1]
    wid = args[15].shape[1]
    heads = args[10].shape[0]
    return (
        n == 8 and m % 2 == 0 and wid % 256 == 0 and ca % 256 == 0 and cr % 128 == 0 and depth % 16 == 0
        and quarter % 32 == 0 and (quarter * m) % 256 == 0 and heads <= 8
    )


def whole_program(*args):
    n = lax.axis_size("sp")
    m = lax.axis_size("tp")
    return fused(*args) if fits(n, m, args) else local(*args)


def solution(mesh):
    return jax.shard_map(
        whole_program,
        mesh=mesh,
        in_specs=(
            P(("sp", "tp"), None),
            P(),
            P("sp", "tp"),
            P("sp", "tp"),
            P("sp", "tp"),
            P("sp", "tp"),
            P(None, "tp"),
            P("tp"),
            P("tp"),
            P(None, "tp"),
            P("tp", None, None),
            P("tp", None, None),
            P("tp"),
            P("sp", "tp"),
            P("tp"),
            P("tp", "sp"),
            P("tp", "sp"),
        ),
        out_specs=P(("sp", "tp"), None),
        check_vma=False,
    )
```
